32 devices in a mesh: grp: 2 (over y), sp: 4 (over z), tp: 4 (over x, core).
Axes of the slice: x: 2, y: 2, z: 4, core: 2. Of those that a mesh axis runs over, the one named last changes fastest.
Arguments:
- residual: bfloat16 [6144, 2048], P(('grp', 'sp', 'tp')), parts along dimension 0, may hold values from -6 to 6
- value_projected: bfloat16 [6144, 4096], P(('grp', 'sp'), 'tp'), parts along dimension 0, may hold values from -6 to 6
- gate_projected: bfloat16 [6144, 4096], P(('grp', 'sp'), 'tp'), parts along dimension 0, may hold values from -6 to 6
- wide_key_rows: bfloat16 [6144, 1024], P(('grp', 'sp'), 'tp'), parts along dimension 0, may hold values from -6 to 6
- wide_query_rows: bfloat16 [6144, 1024], P(('grp', 'sp'), 'tp'), parts along dimension 0, may hold values from -6 to 6
- narrow_key_rows: bfloat16 [6144, 512], P(('grp', 'sp'), 'tp'), parts along dimension 0, may hold values from -6 to 6
- narrow_query_rows: bfloat16 [6144, 512], P(('grp', 'sp'), 'tp'), parts along dimension 0, may hold values from -6 to 6
- step_before_softplus: float32 [6144, 64], P(('grp', 'sp'), 'tp'), parts along dimension 0, may hold values from -5 to 5
- extra_log_decay: float32 [6144, 64], P(('grp', 'sp'), 'tp'), parts along dimension 0, may hold values from -0.7 to 0
- log_decay_rate: float32 [64], P('tp'), may hold values from -12.3 to -2.99
- value_kernel: bfloat16 [4, 4096], P(None, 'tp'), may hold values from -3 to 3
- wide_key_kernel: bfloat16 [4, 1024], P(None, 'tp'), may hold values from -3 to 3
- wide_query_kernel: bfloat16 [4, 1024], P(None, 'tp'), may hold values from -3 to 3
- narrow_key_kernel: bfloat16 [4, 512], P(None, 'tp'), may hold values from -3 to 3
- narrow_query_kernel: bfloat16 [4, 512], P(None, 'tp'), may hold values from -3 to 3
- head_norm_gain: bfloat16 [4096], P('tp'), may hold values from 0.099609375 to 1.8984375
- output_matrix: bfloat16 [4096, 2048], P('tp'), may hold values from -0.09375 to 0.09375
- feedforward_norm_gain: bfloat16 [2048], replicated, may hold values from 0.099609375 to 1.8984375
- gate_matrix: bfloat16 [2048, 3072], P('sp', 'tp'), may hold values from -0.125 to 0.125
- up_matrix: bfloat16 [2048, 3072], P('sp', 'tp'), may hold values from -0.125 to 0.125
- down_matrix: bfloat16 [2048, 3072], P('sp', 'tp'), may hold values from -0.3125 to 0.3125
Outputs:
- mixed: bfloat16 [6144, 2048], P(('grp', 'sp', 'tp')), parts along dimension 0
The draws below stay inside these ranges and needn't reach their ends.
There are 2 independent parts, one for each index of `grp`. The reference program is written for one: setup_inputs(seed, part) draws one part's arguments, and reference() takes and returns one part's arrays. A program takes and returns all parts, laid end to end along the dimension named above; an argument that names none is the same for every part. Nothing has to cross between parts.
All inputs are finite; a program needn't handle non-finite values.
Results may differ from the reference program's by a relative error of at most 0.015.
Values may be sent and summed in bfloat16 or wider, within the bound.
No kernel may reach another device: no remote copies, remote signals or barrier semaphores. Data moves between devices by JAX's collectives and lax.ppermute only.
A program may use at most 128 MiB of HBM per device.

```python
import math
import jax
import jax.numpy as jnp
from jax import lax

D = 2048
HEADS = 64
HEAD_DIM = 64
GROUPS = 16
STATE_WIDE = 128
STATE_NARROW = 64
FF = 3072
CONV_W = 4
BLK = 64
TOK_DEV = 768
INNER = 4096
TOKENS = 3072
N_TP = 4


def draw_step_before_softplus(key, part):
    noise_key, shift_key = jax.random.split(jax.random.fold_in(key, 11))
    count = TOKENS // TOK_DEV
    shifts = jax.random.uniform(shift_key, (count, 1, HEADS), jnp.float32, -1.0, 1.0)
    noise = jnp.clip(jax.random.normal(noise_key, (count, TOK_DEV, HEADS), jnp.float32), -4.0, 4.0)
    return (noise + shifts).reshape(TOKENS, HEADS)


def draw_extra_log_decay(key, part):
    place_key, loss_key = jax.random.split(jax.random.fold_in(key, 23))
    places = jax.random.randint(place_key, (2, HEADS), 0, TOKENS)
    losses = jax.random.uniform(loss_key, (2, HEADS), jnp.float32, 0.2, 0.5)
    positions = jnp.arange(TOKENS, dtype=jnp.int32)[:, None]
    total = jnp.zeros((TOKENS, HEADS), jnp.float32)
    for number in range(2):
        total = total + jnp.where(positions == places[number][None, :], jnp.log(1.0 - losses[number])[None, :], 0.0)
    return total


def draw_log_decay_rate(key, part):
    order_key, slow_key, fast_key = jax.random.split(jax.random.fold_in(key, 37), 3)
    order = jax.random.permutation(order_key, HEADS)
    fast_count = HEADS // 2
    slow = math.log(5e-06) + jax.random.uniform(slow_key, (HEADS,), jnp.float32) * math.log(4.0)
    fast = math.log(0.03) + jax.random.uniform(fast_key, (HEADS,), jnp.float32) * math.log(0.05 / 0.03)
    return jnp.where(order < fast_count, fast, slow)


def steps_of(key, extent, shards, least, top_value):
    level = 1.0
    for position, blocks in shards:
        draws = jax.random.uniform(jax.random.fold_in(jax.random.fold_in(key, 6), position), (blocks,), jnp.float32, least / len(shards), top_value / len(shards))
        level = level * jnp.repeat(jnp.exp(draws), extent[position] // blocks).reshape((-1,) + (1,) * (len(extent) - 1 - position))
    return level


def normal_values(own_key, dims, scale, bound, shards=(), kind=jnp.bfloat16):
    result = jax.random.normal(own_key, dims, jnp.float32) * scale
    if len(shards) > 0:
        result = steps_of(own_key, dims, shards, -0.22, 0.18) * result
    return jnp.clip(result, min=-bound, max=bound).astype(kind)


def setup_inputs(seed: int = 0, part: int = 0) -> dict:
    seeds = jax.random.split(jax.random.key(seed), 22)
    part_keys = jax.random.split(jax.random.fold_in(seeds[21], part), 22)
    return {
        "residual": normal_values(part_keys[0], (TOKENS, D), 1.0, 6.0, ((0, 16),)),
        "value_projected": normal_values(part_keys[1], (TOKENS, INNER), 1.0, 6.0, ((0, 4), (1, 4))),
        "gate_projected": normal_values(part_keys[2], (TOKENS, INNER), 1.0, 6.0, ((0, 4), (1, 4))),
        "wide_key_rows": normal_values(part_keys[3], (TOKENS, GROUPS * STATE_WIDE // 2), 1.0, 6.0, ((0, 4), (1, 4))),
        "wide_query_rows": normal_values(part_keys[4], (TOKENS, GROUPS * STATE_WIDE // 2), 1.0, 6.0, ((0, 4), (1, 4))),
        "narrow_key_rows": normal_values(part_keys[5], (TOKENS, GROUPS * STATE_NARROW // 2), 1.0, 6.0, ((0, 4), (1, 4))),
        "narrow_query_rows": normal_values(part_keys[6], (TOKENS, GROUPS * STATE_NARROW // 2), 1.0, 6.0, ((0, 4), (1, 4))),
        "step_before_softplus": draw_step_before_softplus(jax.random.fold_in(jax.random.fold_in(seeds[21], part), 71), part),
        "extra_log_decay": draw_extra_log_decay(jax.random.fold_in(jax.random.fold_in(seeds[21], part), 71), part),
        "log_decay_rate": draw_log_decay_rate(jax.random.fold_in(seeds[21], 71), part),
        "value_kernel": normal_values(seeds[10], (CONV_W, INNER), CONV_W ** -0.5, 3.0, ((1, 4),)),
        "wide_key_kernel": normal_values(seeds[11], (CONV_W, GROUPS * STATE_WIDE // 2), CONV_W ** -0.5, 3.0, ((1, 4),)),
        "wide_query_kernel": normal_values(seeds[12], (CONV_W, GROUPS * STATE_WIDE // 2), CONV_W ** -0.5, 3.0, ((1, 4),)),
        "narrow_key_kernel": normal_values(seeds[13], (CONV_W, GROUPS * STATE_NARROW // 2), CONV_W ** -0.5, 3.0, ((1, 4),)),
        "narrow_query_kernel": normal_values(seeds[14], (CONV_W, GROUPS * STATE_NARROW // 2), CONV_W ** -0.5, 3.0, ((1, 4),)),
        "head_norm_gain": jnp.clip(1.0 + 0.18 * jax.random.normal(seeds[15], (INNER,), jnp.float32), 0.099609375, 1.8984375).astype(jnp.bfloat16),
        "output_matrix": normal_values(seeds[16], (INNER, D), INNER ** -0.5, 0.09375, ((0, 4),)),
        "feedforward_norm_gain": jnp.clip(1.0 + 0.18 * jax.random.normal(seeds[17], (D,), jnp.float32), 0.099609375, 1.8984375).astype(jnp.bfloat16),
        "gate_matrix": normal_values(seeds[18], (D, FF), D ** -0.5, 0.125, ((0, 4), (1, 4))),
        "up_matrix": normal_values(seeds[19], (D, FF), D ** -0.5, 0.125, ((0, 4), (1, 4))),
        "down_matrix": normal_values(seeds[20], (D, FF), (FF // 9) ** -0.5, 0.3125, ((0, 4), (1, 4))),
    }


def to_half(value):
    return lax.optimization_barrier(value.astype(jnp.bfloat16)).astype(jnp.float32)

def short_conv(inputs, kernel):
    width = kernel.shape[0]
    length = inputs.shape[0]
    padded = jnp.pad(inputs.astype(jnp.float32), ((width - 1, 0), (0, 0)))
    total = jnp.zeros(inputs.shape, jnp.float32)
    for offset in range(width):
        total = total + padded[offset:offset + length] * kernel[offset].astype(jnp.float32)
    return jax.nn.silu(total).astype(jnp.bfloat16)

def family_mix(values, step_sizes, decay_factor, keys, queries):
    length, groups, per_group, width = values.shape
    states = keys.shape[2]
    count = length // BLK
    lower = jnp.tril(jnp.ones((BLK, BLK), dtype=bool))
    highest = lax.Precision.HIGHEST

    def advance(carried, block):
        block_values, block_steps, block_decay, block_keys, block_queries = block
        values32 = block_values.astype(jnp.float32)
        keys32 = block_keys.astype(jnp.float32)
        queries32 = block_queries.astype(jnp.float32)
        running = jnp.cumsum(block_decay, axis=0)
        scores = jnp.einsum('lgn,sgn->lsg', queries32, keys32, precision=highest)
        spread = jnp.where(lower[:, :, None, None], running[:, None] - running[None, :], -jnp.inf)
        weights = to_half(scores[..., None] * jnp.exp(spread) * block_steps[None])
        inside = jnp.einsum('lsgr,sgrp->lgrp', weights, values32, precision=highest)
        outside = jnp.exp(running)[..., None] * jnp.einsum('lgn,grpn->lgrp', queries32, to_half(carried), precision=highest)
        fade = block_steps * jnp.exp(running[-1][None] - running)
        scaled = to_half(values32 * fade[..., None])
        block_state = jnp.einsum('lgrp,lgn->grpn', scaled, keys32, precision=highest)
        carried = jnp.exp(running[-1])[..., None, None] * carried + block_state
        return (carried, inside + outside)
    blocks = (values.reshape(count, BLK, groups, per_group, width), step_sizes.reshape(count, BLK, groups, per_group), decay_factor.reshape(count, BLK, groups, per_group), keys.reshape(count, BLK, groups, states), queries.reshape(count, BLK, groups, states))
    initial = jnp.zeros((groups, per_group, width, states), jnp.float32)
    ending, outputs = lax.scan(advance, initial, blocks)
    return outputs.reshape(length, groups, per_group, width)

def reference(residual, value_projected, gate_projected, wide_key_rows, wide_query_rows, narrow_key_rows, narrow_query_rows, step_before_softplus, extra_log_decay, log_decay_rate, value_kernel, wide_key_kernel, wide_query_kernel, narrow_key_kernel, narrow_query_kernel, head_norm_gain, output_matrix, feedforward_norm_gain, gate_matrix, up_matrix, down_matrix):
    length = value_projected.shape[0]
    per_group = HEADS // GROUPS
    half = GROUPS // 2
    values = short_conv(value_projected, value_kernel).reshape(length, half, 2, per_group, HEAD_DIM)
    keys_w = short_conv(wide_key_rows, wide_key_kernel).reshape(length, half, STATE_WIDE)
    queries_w = short_conv(wide_query_rows, wide_query_kernel).reshape(length, half, STATE_WIDE)
    keys_n = short_conv(narrow_key_rows, narrow_key_kernel).reshape(length, half, STATE_NARROW)
    queries_n = short_conv(narrow_query_rows, narrow_query_kernel).reshape(length, half, STATE_NARROW)
    step_sizes = jax.nn.softplus(step_before_softplus)
    decay_factor = -jnp.exp(log_decay_rate)[None, :] * step_sizes + extra_log_decay
    step_sizes = step_sizes.reshape(length, half, 2, per_group)
    decay_factor = decay_factor.reshape(length, half, 2, per_group)
    wide = family_mix(values[:, :, 0], step_sizes[:, :, 0], decay_factor[:, :, 0], keys_w, queries_w)
    narrow = family_mix(values[:, :, 1], step_sizes[:, :, 1], decay_factor[:, :, 1], keys_n, queries_n)
    heads_out = jnp.stack([wide, narrow], axis=2).reshape(length, HEADS, HEAD_DIM)
    gated = heads_out * jax.nn.silu(gate_projected.astype(jnp.float32)).reshape(length, HEADS, HEAD_DIM)
    gated = gated * lax.rsqrt(lax.optimization_barrier(jnp.mean(gated * gated, axis=-1, keepdims=True)) + 1e-06)
    normed = (gated.reshape(length, INNER) * head_norm_gain.astype(jnp.float32)).astype(jnp.bfloat16)
    share = INNER // N_TP
    projected = jnp.zeros((length, D), jnp.float32)
    for index in range(N_TP):
        partial_value = jnp.dot(normed[:, index * share:(index + 1) * share], output_matrix[index * share:(index + 1) * share], preferred_element_type=jnp.float32)
        projected = projected + to_half(partial_value)
    after_mixer = (residual.astype(jnp.float32) + projected).astype(jnp.bfloat16)
    rows = after_mixer.astype(jnp.float32)
    x_norm = (rows * lax.rsqrt(lax.optimization_barrier(jnp.mean(rows * rows, axis=-1, keepdims=True)) + 1e-06) * feedforward_norm_gain.astype(jnp.float32)).astype(jnp.bfloat16)
    gate_values = jnp.dot(x_norm, gate_matrix, preferred_element_type=jnp.float32)
    up_values = jnp.dot(x_norm, up_matrix, preferred_element_type=jnp.float32)
    hidden = (jax.nn.silu(gate_values) * up_values).astype(jnp.bfloat16)
    portion = FF // N_TP
    channel = jnp.zeros((length, D), jnp.float32)
    for index in range(N_TP):
        partial_value = lax.dot_general(hidden[:, index * portion:(index + 1) * portion], down_matrix[:, index * portion:(index + 1) * portion], (((1,), (1,)), ((), ())), preferred_element_type=jnp.float32)
        channel = channel + to_half(partial_value)
    return (after_mixer.astype(jnp.float32) + 0.5 * channel).astype(jnp.bfloat16)
```

```python
import functools
import jax
import jax.numpy as jnp
from jax import lax
from jax.experimental import pallas as pl
from jax.experimental.pallas import tpu as pltpu
from jax.sharding import PartitionSpec as P


HEAD_DIM = 64
PER_GROUP = 4
GROUP_COLS = HEAD_DIM * PER_GROUP
STATE_WIDE = 128
STATE_NARROW = 64
CHUNK = 128
TAIL = 16
FADE_ROWS = 16
F32 = jnp.float32
BF16 = jnp.bfloat16


def silu(x):
    half = 0.5 * x
    return half + half * jnp.tanh(half)


def spread(values, table):
    high = values.astype(BF16).astype(F32)
    low = values - high
    return jnp.dot(
        jnp.concatenate([high, low], axis=1).astype(BF16), table, preferred_element_type=F32
    )


def head_table(heads, columns):
    head = lax.broadcasted_iota(jnp.int32, (2 * heads, columns), 0)
    head = jnp.where(head >= heads, head - heads, head)
    column = lax.broadcasted_iota(jnp.int32, (2 * heads, columns), 1)
    inside = (column >= head * HEAD_DIM) & (column < (head + 1) * HEAD_DIM)
    return jnp.where(inside, 1.0, 0.0).astype(BF16)


def narrow_mask(place, rows, lanes):
    lane = lax.broadcasted_iota(jnp.int32, (rows, lanes), 1)
    start = place * STATE_NARROW
    return (lane >= start) & (lane < start + STATE_NARROW)


def tails_body(*refs):
    out_ref = refs[-1]
    offset = 0
    for ref in refs[:-1]:
        out_ref[:, offset : offset + ref.shape[1]] = ref[...]
        offset += ref.shape[1]


def tails_call(raw):
    length = raw[0].shape[0]
    width = sum(a.shape[1] for a in raw)
    return pl.pallas_call(
        tails_body,
        grid=(1,),
        in_specs=[
            pl.BlockSpec((TAIL, a.shape[1]), lambda i: (length // TAIL - 1, 0)) for a in raw
        ],
        out_specs=pl.BlockSpec((TAIL, width), lambda i: (0, 0)),
        out_shape=jax.ShapeDtypeStruct((TAIL, width), BF16),
        name="tails",
    )(*raw)


def local_body(
    value_ref,
    kw_ref,
    qw_ref,
    kn_ref,
    qn_ref,
    step_ref,
    extra_ref,
    rate_ref,
    rim_ref,
    value_taps,
    kw_taps,
    qw_taps,
    kn_taps,
    qn_taps,
    y_ref,
    q_ref,
    fade_ref,
    state_ref,
    raw,
    carried,
    before,
):
    turn = pl.program_id(0)
    chunk = value_ref.shape[0]
    heads = step_ref.shape[0]
    columns = value_ref.shape[1]
    table = head_table(heads, columns)

    @pl.when(turn == 0)
    def _():
        raw[0:8, :] = rim_ref[...].astype(F32)[TAIL - 8 :, :]
        carried[...] = jnp.zeros_like(carried)
        before[...] = jnp.zeros_like(before)

    @pl.when(turn > 0)
    def _():
        raw[0:8, :] = raw[chunk : chunk + 8, :]

    starts = []
    offset = 0
    for ref in (value_ref, kw_ref, qw_ref, kn_ref, qn_ref):
        starts.append(offset)
        raw[8 : 8 + chunk, offset : offset + ref.shape[1]] = ref[...].astype(F32)
        offset += ref.shape[1]

    def conv(which, start, width):
        taps_ref = (value_taps, kw_taps, qw_taps, kn_taps, qn_taps)[which]
        weights = taps_ref[:, start : start + width].astype(F32)
        taps = weights.shape[0]
        start = starts[which] + start
        total = None
        for tap in range(taps):
            first = 8 - (taps - 1) + tap
            term = raw[first : first + chunk, start : start + width] * weights[tap : tap + 1]
            total = term if total is None else total + term
        return silu(total).astype(BF16)

    step = jnp.log(1.0 + jnp.exp(step_ref[...].T))
    decay = extra_ref[...].T - jnp.exp(rate_ref[...]) * step
    row = lax.broadcasted_iota(jnp.int32, (chunk, chunk), 0)
    column = lax.broadcasted_iota(jnp.int32, (chunk, chunk), 1)
    lower = row >= column
    first = decay.astype(BF16).astype(F32)
    second = (decay - first).astype(BF16).astype(F32)
    terms = jnp.concatenate([first, second, decay - first - second], axis=1).astype(BF16)
    sums = jnp.dot(
        jnp.where(lower, 1.0, 0.0).astype(BF16), terms, preferred_element_type=F32
    )
    running = sums[:, :heads] + sums[:, heads : 2 * heads] + sums[:, 2 * heads :]
    middle = running[chunk // 2 - 1 : chunk // 2, :]
    total = running[chunk - 1 : chunk, :]
    since = jnp.exp(running)
    fade_ref[...] = jnp.exp(running + before[0:1, :])
    before[...] = before[...] + total
    factors = spread(
        jnp.concatenate(
            [
                jnp.exp(middle - running) * step,
                jnp.exp(running - middle),
                since[chunk // 2 - 8 : chunk // 2],
                since[chunk - 8 : chunk],
            ],
            axis=0,
        ),
        table,
    )
    to_middle = factors[:chunk]
    from_middle = factors[chunk : 2 * chunk]
    at_middle = factors[2 * chunk + 7 : 2 * chunk + 8, :]
    at_end = factors[2 * chunk + 15 : 2 * chunk + 16, :]
    middle_to_end = from_middle[chunk - 1 : chunk, :]

    groups = columns // GROUP_COLS
    for group in range(groups):
        place = group // 2
        lanes = slice(group * GROUP_COLS, (group + 1) * GROUP_COLS)
        values = conv(0, group * GROUP_COLS, GROUP_COLS)
        scaled = (values.astype(F32) * to_middle[:, lanes]).astype(BF16)
        if group % 2 == 0:
            keys = conv(1, place * STATE_WIDE, STATE_WIDE)
            queries = conv(2, place * STATE_WIDE, STATE_WIDE)
            q_ref[:, place * STATE_WIDE : (place + 1) * STATE_WIDE] = queries
        else:
            pair = place // 2
            inner = place % 2
            if inner == 0:
                keys_n = conv(3, pair * STATE_WIDE, STATE_WIDE)
                queries_n = conv(4, pair * STATE_WIDE, STATE_WIDE)
                first = kw_ref.shape[1] + pair * STATE_WIDE
                q_ref[:, first : first + STATE_WIDE] = queries_n
            mask = narrow_mask(inner, chunk, STATE_WIDE)
            keys = jnp.where(mask, keys_n, jnp.zeros_like(keys_n))
            queries = queries_n
        scores = lax.dot_general(
            queries, keys, (((1,), (1,)), ((), ())), preferred_element_type=F32
        )
        scores = jnp.where(lower, scores, 0.0).astype(BF16)
        state = carried[group]
        entering = (state * at_middle[:, lanes]).astype(BF16)
        mixed = jnp.dot(
            jnp.concatenate([scores, queries], axis=1),
            jnp.concatenate([scaled, entering], axis=0),
            preferred_element_type=F32,
        )
        y_ref[:, lanes] = mixed * from_middle[:, lanes]
        gained = lax.dot_general(
            keys, scaled, (((0,), (0,)), ((), ())), preferred_element_type=F32
        )
        carried[group] = state * at_end[:, lanes] + gained * middle_to_end[:, lanes]

    @pl.when(turn == pl.num_programs(0) - 1)
    def _():
        whole = spread(jnp.exp(before[...]), table)
        wide = (groups // 2) * STATE_WIDE
        last = state_ref.shape[0] - FADE_ROWS
        row = lax.broadcasted_iota(jnp.int32, (FADE_ROWS, GROUP_COLS), 0)
        fades = jnp.zeros((FADE_ROWS, GROUP_COLS), F32)
        for group in range(groups):
            place = group // 2
            lanes = slice(group * GROUP_COLS, (group + 1) * GROUP_COLS)
            fades = jnp.where(row == group, whole[0:1, lanes], fades)
            if group % 2 == 0:
                at = place * STATE_WIDE
                state_ref[at : at + STATE_WIDE, :] = carried[group].astype(BF16)
            else:
                inner = (place % 2) * STATE_NARROW
                at = wide + place * STATE_NARROW
                state_ref[at : at + STATE_NARROW, :] = carried[group][
                    inner : inner + STATE_NARROW, :
                ].astype(BF16)
        state_ref[last:, :] = fades.astype(BF16)


def joined(later, earlier):
    last = later.shape[0] - FADE_ROWS
    groups = last // (STATE_WIDE + STATE_NARROW) * 2
    wide = (groups // 2) * STATE_WIDE
    later, earlier = later.astype(F32), earlier.astype(F32)
    parts = []
    for place in range(groups // 2):
        rows = slice(place * STATE_WIDE, (place + 1) * STATE_WIDE)
        fade = later[last + 2 * place : last + 2 * place + 1]
        parts.append(fade * earlier[rows] + later[rows])
    for place in range(groups // 2):
        rows = slice(wide + place * STATE_NARROW, wide + (place + 1) * STATE_NARROW)
        fade = later[last + 2 * place + 1 : last + 2 * place + 2]
        parts.append(fade * earlier[rows] + later[rows])
    parts.append(later[last:] * earlier[last:])
    return jnp.concatenate(parts, axis=0).astype(BF16)


def join_body(later_ref, earlier_ref, out_ref):
    out_ref[...] = joined(later_ref[...], earlier_ref[...])


def join_call(later, earlier):
    return pl.pallas_call(
        join_body, out_shape=jax.ShapeDtypeStruct(later.shape, BF16), name="join_states"
    )(later, earlier)


def final_body(
    ids_ref, y_ref, q_ref, fade_ref, gate_ref, gain_ref, near_ref, far_ref, matrix_ref, out_ref, state, normed, matrix, arrived
):
    rows, columns = y_ref.shape
    heads = fade_ref.shape[1]
    table = head_table(heads, columns)
    turn = pl.program_id(0)
    copy = pltpu.make_async_copy(matrix_ref, matrix, arrived)

    @pl.when(turn == 0)
    def _():
        copy.start()
        state[...] = joined(near_ref[...], far_ref[...])

    fade = spread(fade_ref[...], table)
    groups = columns // GROUP_COLS
    wide = (groups // 2) * STATE_WIDE
    parts = []
    squares = []
    for group in range(groups):
        place = group // 2
        lanes = slice(group * GROUP_COLS, (group + 1) * GROUP_COLS)
        if group % 2 == 0:
            at = place * STATE_WIDE
            queries = q_ref[:, at : at + STATE_WIDE]
        else:
            at = wide + (place // 2) * STATE_WIDE
            queries = q_ref[:, at : at + STATE_WIDE]
            queries = jnp.where(
                narrow_mask(place % 2, rows, STATE_WIDE), queries, jnp.zeros_like(queries)
            )
        outer = jnp.dot(queries, state[at : at + STATE_WIDE, :], preferred_element_type=F32)
        mixed = y_ref[:, lanes] + outer * fade[:, lanes]
        gated = mixed * silu(gate_ref[:, lanes].astype(F32))
        parts.append(gated)
        square = (gated * gated).astype(BF16)
        squares.append(
            lax.dot_general(
                square,
                table[0:heads, lanes],
                (((1,), (1,)), ((), ())),
                preferred_element_type=F32,
            )
        )
    mean = functools.reduce(jnp.add, squares) * (1.0 / HEAD_DIM)
    scale = spread(lax.rsqrt(mean + 1e-06), table)
    at = pl.multiple_of(turn * rows, rows)
    for group in range(groups):
        lanes = slice(group * GROUP_COLS, (group + 1) * GROUP_COLS)
        gain = gain_ref[0:1, lanes].astype(F32)
        normed[pl.ds(at, rows), lanes] = (parts[group] * scale[:, lanes] * gain).astype(BF16)

    @pl.when(turn == pl.num_programs(0) - 1)
    def _():
        copy.wait()
        width = out_ref.shape[1]
        step = 512
        for start in range(0, width, step):
            product = jnp.dot(
                normed[...], matrix[:, start : start + step], preferred_element_type=F32
            )
            out_ref[:, start : start + step] = product.astype(out_ref.dtype)


def local_call(raw, step, extra, rate, rim, taps):
    length, columns = raw[0].shape
    heads = step.shape[0]
    chunk = CHUNK
    groups = columns // GROUP_COLS
    width = rim.shape[1]
    states = raw[1].shape[1] + raw[3].shape[1]

    def rows(array):
        return pl.BlockSpec((chunk, array.shape[1]), lambda i: (i, 0))

    def fixed(shape):
        return pl.BlockSpec(shape, lambda i: tuple(0 for _ in shape))

    turned = pl.BlockSpec((heads, chunk), lambda i: (0, i))
    return pl.pallas_call(
        local_body,
        grid=(length // chunk,),
        in_specs=[rows(a) for a in raw]
        + [turned, turned, fixed(rate.shape), fixed(rim.shape)]
        + [fixed(t.shape) for t in taps],
        out_specs=[
            pl.BlockSpec((chunk, columns), lambda i: (i, 0)),
            pl.BlockSpec((chunk, states), lambda i: (i, 0)),
            pl.BlockSpec((chunk, heads), lambda i: (i, 0)),
            fixed((states + FADE_ROWS, GROUP_COLS)),
        ],
        out_shape=[
            jax.ShapeDtypeStruct((length, columns), F32),
            jax.ShapeDtypeStruct((length, states), BF16),
            jax.ShapeDtypeStruct((length, heads), F32),
            jax.ShapeDtypeStruct((states + FADE_ROWS, GROUP_COLS), BF16),
        ],
        scratch_shapes=[
            pltpu.VMEM((8 + chunk, width), F32),
            pltpu.VMEM((groups, STATE_WIDE, GROUP_COLS), F32),
            pltpu.VMEM((8, heads), F32),
        ],
        compiler_params=pltpu.CompilerParams(dimension_semantics=("arbitrary",)),
        cost_estimate=pl.CostEstimate(
            flops=12_000_000_000, bytes_accessed=10_000_000, transcendentals=0
        ),
        name="mix_local",
    )(*raw, step, extra, rate, rim, *taps)


def final_call(ids, y, q, fade, gate, gain, near, far, matrix, rows_each, kind):
    columns = y.shape[1]
    width = matrix.shape[1]
    count = ids.shape[0]

    def rows(array):
        return pl.BlockSpec((rows_each, array.shape[1]), lambda i, ids: (ids[i], 0))

    def fixed(array):
        return pl.BlockSpec(array.shape, lambda i, ids: (0, 0))

    return pl.pallas_call(
        final_body,
        grid_spec=pltpu.PrefetchScalarGridSpec(
            num_scalar_prefetch=1,
            grid=(count,),
            in_specs=[rows(y), rows(q), rows(fade), rows(gate)]
            + [fixed(a) for a in (gain, near, far)]
            + [pl.BlockSpec(memory_space=pl.ANY)],
            out_specs=pl.BlockSpec((rows_each * count, width), lambda i, ids: (0, 0)),
            scratch_shapes=[
                pltpu.VMEM(near.shape, BF16),
                pltpu.VMEM((rows_each * count, columns), BF16),
                pltpu.VMEM(matrix.shape, BF16),
                pltpu.SemaphoreType.DMA,
            ],
        ),
        out_shape=jax.ShapeDtypeStruct((rows_each * count, width), kind),
        compiler_params=pltpu.CompilerParams(dimension_semantics=("arbitrary",)),
        cost_estimate=pl.CostEstimate(
            flops=6_000_000_000, bytes_accessed=10_000_000, transcendentals=0
        ),
        name="mix_final",
    )(ids, y, q, fade, gate, gain, near, far, matrix)


def settle_body(residual_ref, kept_ref, near_ref, far_ref, gain_ref, after_ref, norm_ref):
    total = kept_ref[...] + near_ref[...].astype(F32) + far_ref[...].astype(F32)
    after = (residual_ref[...].astype(F32) + total).astype(BF16)
    after_ref[...] = after
    wide = after.astype(F32)
    mean = jnp.mean(wide * wide, axis=-1, keepdims=True)
    norm_ref[...] = (wide * lax.rsqrt(mean + 1e-06) * gain_ref[...].astype(F32)).astype(BF16)


def settle_call(residual, kept, near, far, gain):
    rows, width = residual.shape
    top = pl.BlockSpec((rows // 2, width), lambda i: (i, 0))
    return pl.pallas_call(
        settle_body,
        grid=(2,),
        in_specs=[top] * 4 + [pl.BlockSpec(gain.shape, lambda i: (0, 0))],
        out_specs=[top, top],
        out_shape=[jax.ShapeDtypeStruct(residual.shape, BF16)] * 2,
        name="settle",
    )(residual, kept, near, far, gain)


def finish_body(after_ref, kept_ref, came_ref, l1_ref, l2_ref, r1_ref, r2_ref, out_ref):
    half = l1_ref.shape[1]
    share = kept_ref[...].astype(F32) + came_ref[...].astype(F32)
    left = share[:, :half] + l1_ref[...].astype(F32) + l2_ref[...].astype(F32)
    right = share[:, half:] + r1_ref[...].astype(F32) + r2_ref[...].astype(F32)
    out_ref[:, :half] = (after_ref[:, :half].astype(F32) + 0.5 * left).astype(BF16)
    out_ref[:, half:] = (after_ref[:, half:].astype(F32) + 0.5 * right).astype(BF16)


def finish_call(*arrays):
    rows, width = arrays[0].shape
    each = rows // 2
    return pl.pallas_call(
        finish_body,
        grid=(2,),
        in_specs=[pl.BlockSpec((each, a.shape[1]), lambda i: (i, 0)) for a in arrays],
        out_specs=pl.BlockSpec((each, width), lambda i: (i, 0)),
        out_shape=jax.ShapeDtypeStruct((rows, width), BF16),
        name="finish",
    )(*arrays)


def pick_body(part_ref, gate_ref, up_ref, down_ref, out_ref):
    columns = gate_ref.shape[1]
    for k, ref in enumerate((gate_ref, up_ref, down_ref)):
        out_ref[:, k * columns : (k + 1) * columns] = ref[...]


def pick_call(part, parts, weights):
    rows, columns = weights[0].shape
    columns //= parts
    return pl.pallas_call(
        pick_body,
        grid_spec=pltpu.PrefetchScalarGridSpec(
            num_scalar_prefetch=1,
            grid=(1,),
            in_specs=[pl.BlockSpec((rows, columns), lambda i, part: (0, part[0]))] * 3,
            out_specs=pl.BlockSpec((rows, 3 * columns), lambda i, part: (0, 0)),
        ),
        out_shape=jax.ShapeDtypeStruct((rows, 3 * columns), BF16),
        name="pick",
    )(part, *weights)


def feed_body(*refs):
    out_refs = refs[-4:-2]
    total, downs = refs[-2:]
    x_refs, weight_ref = refs[:-5], refs[-5]
    step = pl.program_id(0)
    depth = weight_ref.shape[0]
    columns = weight_ref.shape[1] // 3

    @pl.when(step == 0)
    def _():
        total[...] = jnp.zeros_like(total)

    downs[pl.ds(pl.multiple_of(step * depth, depth), depth), :] = weight_ref[:, 2 * columns :]
    x = jnp.concatenate([x_ref[...] for x_ref in x_refs], axis=0)
    total[...] += jnp.dot(x, weight_ref[:, : 2 * columns], preferred_element_type=F32)

    @pl.when(step == pl.num_programs(0) - 1)
    def _():
        rows, width = out_refs[0].shape
        hidden = (silu(total[:, :columns]) * total[:, columns:]).astype(BF16)
        for start in range(0, width, 512):
            product = lax.dot_general(
                hidden,
                downs[start : start + 512, :],
                (((1,), (1,)), ((), ())),
                preferred_element_type=F32,
            ).astype(BF16)
            out_refs[0][:, start : start + 512] = product[:rows]
            out_refs[1][:, start : start + 512] = product[rows:]


def feed_call(kept, away, weight):
    width = kept[0].shape[1]
    columns = weight.shape[1] // 3
    steps = 4
    depth = width // steps
    rows = sum(a.shape[0] for a in kept)
    outs = jax.ShapeDtypeStruct((rows, width), BF16)
    return pl.pallas_call(
        feed_body,
        grid=(steps,),
        in_specs=[pl.BlockSpec((a.shape[0], depth), lambda k: (0, k)) for a in (*kept, *away)]
        + [pl.BlockSpec((depth, 3 * columns), lambda k: (k, 0))],
        out_specs=[pl.BlockSpec((rows, width), lambda k: (0, 0))] * 2,
        out_shape=[outs, outs],
        scratch_shapes=[
            pltpu.VMEM((2 * rows, 2 * columns), F32),
            pltpu.VMEM((width, columns), BF16),
        ],
        compiler_params=pltpu.CompilerParams(dimension_semantics=("arbitrary",)),
        cost_estimate=pl.CostEstimate(
            flops=12 * rows * width * columns, bytes_accessed=8_000_000, transcendentals=0
        ),
        name="feed",
    )(*kept, *away, weight)


def halves_body(ref, came, left, right):
    half = left.shape[1]
    both = ref[...].astype(F32) + came[...].astype(F32)
    left[...] = both[:, :half].astype(BF16)
    right[...] = both[:, half:].astype(BF16)


def halves_call(*arrays):
    rows, width = arrays[0].shape
    return pl.pallas_call(
        halves_body,
        out_shape=[jax.ShapeDtypeStruct((rows, width // 2), BF16)] * 2,
        name="halves",
    )(*arrays)


def feed_forward(x_norm, after_mixer, weight):
    rows, _ = x_norm.shape
    half = rows // 2

    x1 = x_norm
    x_side = swapped(x1, "tp", 2)
    y_side = swapped(x1, "grp", 1)
    x1_away = swapped(x1, "tp", 1)
    corner_top = swapped(y_side[:half], "tp", 2)
    corner_low = swapped(x_side[half:], "grp", 1)
    x_away = swapped(x_side, "tp", 1)
    y_away = swapped(y_side, "tp", 1)
    top_away = swapped(corner_top, "tp", 1)
    low_away = swapped(corner_low, "tp", 1)

    def feed(kept, away):
        mine, theirs = feed_call(kept, away, weight)
        return mine, swapped(theirs, "tp", 1)

    own, own_came = feed([x1], [x1_away])
    xs, xs_came = feed([x_side], [x_away])
    ys, ys_came = feed([y_side], [y_away])
    corner, corner_came = feed([corner_top, corner_low], [top_away, low_away])
    x_left, x_right = halves_call(xs, xs_came)
    y_left, y_right = halves_call(ys, ys_came)
    l1 = swapped(x_left, "tp", 2)
    r1 = swapped(y_right, "grp", 1)
    c_left, c_right = halves_call(corner, corner_came)
    l2 = swapped(c_left, "tp", 2)
    r2 = swapped(c_right, "grp", 1)
    y_left = (y_left.astype(F32) + l2.astype(F32)).astype(BF16)
    x_right = (x_right.astype(F32) + r2.astype(F32)).astype(BF16)
    l2 = swapped(y_left, "grp", 1)
    r2 = swapped(x_right, "tp", 2)
    return finish_call(after_mixer, own, own_came, l1, l2, r1, r2)


def feed_forward_any(x_norm, after_mixer, weight):
    columns = weight.shape[1] // 3
    x = lax.all_gather(x_norm, ("grp", "tp"), axis=0, tiled=True)
    gates = jnp.dot(x, weight[:, :columns], preferred_element_type=F32)
    ups = jnp.dot(x, weight[:, columns : 2 * columns], preferred_element_type=F32)
    hidden = (silu(gates) * ups).astype(BF16)
    share = lax.dot_general(
        hidden,
        weight[:, 2 * columns :],
        (((1,), (1,)), ((), ())),
        preferred_element_type=F32,
    ).astype(BF16)
    share = lax.psum_scatter(share, ("grp", "tp"), scatter_dimension=0, tiled=True)
    return (after_mixer.astype(F32) + 0.5 * share.astype(F32)).astype(BF16)


def shifted(value, axis, steps):
    count = lax.axis_size(axis)
    return lax.ppermute(value, axis, [(s, s + steps) for s in range(count - steps)])


def swapped(value, axis, bit):
    count = lax.axis_size(axis)
    return lax.ppermute(value, axis, [(s, s ^ bit) for s in range(count)])


def entering_states(packed, axis):
    count = lax.axis_size(axis)
    window, before, got = packed, None, jnp.zeros_like(packed)
    reach = 1
    while reach < count:
        if reach > 1:
            window = join_call(window, got)
            before = got if before is None else join_call(before, got)
        got = shifted(window, axis, reach)
        reach *= 2
    return (got, jnp.zeros_like(got)) if before is None else (before, got)


def on_device(
    residual,
    value_projected,
    gate_projected,
    wide_key_rows,
    wide_query_rows,
    narrow_key_rows,
    narrow_query_rows,
    step_before_softplus,
    extra_log_decay,
    log_decay_rate,
    value_kernel,
    wide_key_kernel,
    wide_query_kernel,
    narrow_key_kernel,
    narrow_query_kernel,
    head_norm_gain,
    output_matrix,
    feedforward_norm_gain,
    gate_matrix,
    up_matrix,
    down_matrix,
):
    members = lax.axis_size("tp")
    place = lax.axis_index("tp")
    part = jnp.reshape(lax.axis_index("grp"), (1,))
    mine = pick_call(part, lax.axis_size("grp"), (gate_matrix, up_matrix, down_matrix))
    raw = (value_projected, wide_key_rows, wide_query_rows, narrow_key_rows, narrow_query_rows)
    tails, mine = lax.optimization_barrier((tails_call(raw), mine))
    rim = shifted(tails, "sp", 1)
    weight = lax.all_gather(mine, "sp", axis=0, tiled=True)

    taps = (
        value_kernel,
        wide_key_kernel,
        wide_query_kernel,
        narrow_key_kernel,
        narrow_query_kernel,
    )
    y, q, fade, packed = local_call(
        raw, step_before_softplus.T, extra_log_decay.T, log_decay_rate[None, :], rim, taps
    )
    near, far = entering_states(packed, "sp")
    rows = y.shape[0] // members
    masks = 2 * jnp.arange(members // 2, dtype=jnp.int32)
    shared = (y, q, fade, gate_projected, head_norm_gain[None, :], near, far, output_matrix, rows)
    away = final_call((place ^ 1) ^ masks, *shared, BF16)
    came = swapped(away, "tp", 1)
    kept = final_call(place ^ masks, *shared, F32)
    bit = members // 2
    total = {m: None for m in range(0, members, 2)}

    def block(array, mask):
        return array[mask // 2 * rows : (mask // 2 + 1) * rows]

    for mask in range(2, members, 2):
        total[mask] = block(kept, mask) + block(came, mask).astype(F32)
    last = None
    while bit > 1:
        for mask in range(0, bit, 2):
            got = swapped(total[mask + bit].astype(BF16), "tp", bit)
            if mask == 0:
                last = got if last is None else last.astype(F32) + got.astype(F32)
            else:
                total[mask] = total[mask] + got.astype(F32)
        bit //= 2
    after_mixer, x_norm = settle_call(residual, kept, came, last, feedforward_norm_gain[None, :])
    if members == 4 and lax.axis_size("grp") == 2:
        return feed_forward(x_norm, after_mixer, weight)
    return feed_forward_any(x_norm, after_mixer, weight)


def solution(mesh):
    in_specs = (
        P(("grp", "sp", "tp"), None),
        P(("grp", "sp"), "tp"),
        P(("grp", "sp"), "tp"),
        P(("grp", "sp"), "tp"),
        P(("grp", "sp"), "tp"),
        P(("grp", "sp"), "tp"),
        P(("grp", "sp"), "tp"),
        P(("grp", "sp"), "tp"),
        P(("grp", "sp"), "tp"),
        P("tp"),
        P(None, "tp"),
        P(None, "tp"),
        P(None, "tp"),
        P(None, "tp"),
        P(None, "tp"),
        P("tp"),
        P("tp", None),
        P(),
        P("sp", "tp"),
        P("sp", "tp"),
        P("sp", "tp"),
    )
    out_specs = P(("grp", "sp", "tp"), None)

    return jax.shard_map(
        on_device, mesh=mesh, in_specs=in_specs, out_specs=out_specs, check_vma=False
    )
```

```python
import functools
import jax
import jax.numpy as jnp
from jax import lax
from jax.experimental import pallas as pl
from jax.experimental.pallas import tpu as pltpu
from jax.sharding import PartitionSpec as P


HEAD_DIM = 64
PER_GROUP = 4
GROUP_COLS = HEAD_DIM * PER_GROUP
STATE_WIDE = 128
STATE_NARROW = 64
CHUNK = 128
TAIL = 16
FADE_ROWS = 16
VMEM_LIMIT = 16 * 1024 * 1024
F32 = jnp.float32
BF16 = jnp.bfloat16


def silu(x):
    half = 0.5 * x
    return half + half * jnp.tanh(half)


def spread(values, table):
    high = values.astype(BF16).astype(F32)
    low = values - high
    return jnp.dot(
        jnp.concatenate([high, low], axis=1).astype(BF16), table, preferred_element_type=F32
    )


def head_table(heads, columns):
    head = lax.broadcasted_iota(jnp.int32, (2 * heads, columns), 0)
    head = jnp.where(head >= heads, head - heads, head)
    column = lax.broadcasted_iota(jnp.int32, (2 * heads, columns), 1)
    inside = (column >= head * HEAD_DIM) & (column < (head + 1) * HEAD_DIM)
    return jnp.where(inside, 1.0, 0.0).astype(BF16)


def narrow_mask(place, rows, lanes):
    lane = lax.broadcasted_iota(jnp.int32, (rows, lanes), 1)
    start = place * STATE_NARROW
    return (lane >= start) & (lane < start + STATE_NARROW)


def tails_body(*refs):
    out_ref, arrived = refs[-2:]
    copies = []
    offset = 0
    for k, ref in enumerate(refs[:-2]):
        rows, columns = ref.shape
        copies.append(
            pltpu.make_async_copy(
                ref.at[rows - TAIL :, :], out_ref.at[:, offset : offset + columns], arrived.at[k]
            )
        )
        offset += columns
    for copy in copies:
        copy.start()
    for copy in copies:
        copy.wait()


def tails_call(raw):
    width = sum(a.shape[1] for a in raw)
    return pl.pallas_call(
        tails_body,
        in_specs=[pl.BlockSpec(memory_space=pltpu.HBM)] * len(raw),
        out_specs=pl.BlockSpec(memory_space=pltpu.VMEM),
        out_shape=jax.ShapeDtypeStruct((TAIL, width), BF16),
        scratch_shapes=[pltpu.SemaphoreType.DMA((len(raw),))],
        name="tails",
    )(*raw)


def local_body(
    value_ref,
    kw_ref,
    qw_ref,
    kn_ref,
    qn_ref,
    step_ref,
    extra_ref,
    rate_ref,
    rim_ref,
    value_taps,
    kw_taps,
    qw_taps,
    kn_taps,
    qn_taps,
    y_ref,
    q_ref,
    fade_ref,
    state_ref,
    raw,
    carried,
    before,
):
    turn = pl.program_id(0)
    chunk = value_ref.shape[0]
    heads = step_ref.shape[0]
    columns = value_ref.shape[1]
    table = head_table(heads, columns)

    @pl.when(turn == 0)
    def _():
        raw[0:8, :] = rim_ref[...].astype(F32)[TAIL - 8 :, :]
        carried[...] = jnp.zeros_like(carried)
        before[...] = jnp.zeros_like(before)

    @pl.when(turn > 0)
    def _():
        raw[0:8, :] = raw[chunk : chunk + 8, :]

    starts = []
    offset = 0
    for ref in (value_ref, kw_ref, qw_ref, kn_ref, qn_ref):
        starts.append(offset)
        raw[8 : 8 + chunk, offset : offset + ref.shape[1]] = ref[...].astype(F32)
        offset += ref.shape[1]

    def conv(which, start, width):
        taps_ref = (value_taps, kw_taps, qw_taps, kn_taps, qn_taps)[which]
        weights = taps_ref[:, start : start + width].astype(F32)
        taps = weights.shape[0]
        start = starts[which] + start
        total = None
        for tap in range(taps):
            first = 8 - (taps - 1) + tap
            term = raw[first : first + chunk, start : start + width] * weights[tap : tap + 1]
            total = term if total is None else total + term
        return silu(total).astype(BF16)

    step = jnp.log(1.0 + jnp.exp(step_ref[...].T))
    decay = extra_ref[...].T - jnp.exp(rate_ref[...]) * step
    row = lax.broadcasted_iota(jnp.int32, (chunk, chunk), 0)
    column = lax.broadcasted_iota(jnp.int32, (chunk, chunk), 1)
    lower = row >= column
    first = decay.astype(BF16).astype(F32)
    second = (decay - first).astype(BF16).astype(F32)
    terms = jnp.concatenate([first, second, decay - first - second], axis=1).astype(BF16)
    sums = jnp.dot(
        jnp.where(lower, 1.0, 0.0).astype(BF16), terms, preferred_element_type=F32
    )
    running = sums[:, :heads] + sums[:, heads : 2 * heads] + sums[:, 2 * heads :]
    middle = running[chunk // 2 - 1 : chunk // 2, :]
    total = running[chunk - 1 : chunk, :]
    since = jnp.exp(running)
    fade_ref[...] = jnp.exp(running + before[0:1, :])
    before[...] = before[...] + total
    factors = spread(
        jnp.concatenate(
            [
                jnp.exp(middle - running) * step,
                jnp.exp(running - middle),
                since[chunk // 2 - 8 : chunk // 2],
                since[chunk - 8 : chunk],
            ],
            axis=0,
        ),
        table,
    )
    to_middle = factors[:chunk]
    from_middle = factors[chunk : 2 * chunk]
    at_middle = factors[2 * chunk + 7 : 2 * chunk + 8, :]
    at_end = factors[2 * chunk + 15 : 2 * chunk + 16, :]
    middle_to_end = from_middle[chunk - 1 : chunk, :]

    groups = columns // GROUP_COLS
    for group in range(groups):
        place = group // 2
        lanes = slice(group * GROUP_COLS, (group + 1) * GROUP_COLS)
        values = conv(0, group * GROUP_COLS, GROUP_COLS)
        scaled = (values.astype(F32) * to_middle[:, lanes]).astype(BF16)
        if group % 2 == 0:
            keys = conv(1, place * STATE_WIDE, STATE_WIDE)
            queries = conv(2, place * STATE_WIDE, STATE_WIDE)
            q_ref[:, place * STATE_WIDE : (place + 1) * STATE_WIDE] = queries
        else:
            pair = place // 2
            inner = place % 2
            if inner == 0:
                keys_n = conv(3, pair * STATE_WIDE, STATE_WIDE)
                queries_n = conv(4, pair * STATE_WIDE, STATE_WIDE)
                first = kw_ref.shape[1] + pair * STATE_WIDE
                q_ref[:, first : first + STATE_WIDE] = queries_n
            mask = narrow_mask(inner, chunk, STATE_WIDE)
            keys = jnp.where(mask, keys_n, jnp.zeros_like(keys_n))
            queries = queries_n
        scores = lax.dot_general(
            queries, keys, (((1,), (1,)), ((), ())), preferred_element_type=F32
        )
        scores = jnp.where(lower, scores, 0.0).astype(BF16)
        state = carried[group]
        entering = (state * at_middle[:, lanes]).astype(BF16)
        mixed = jnp.dot(
            jnp.concatenate([scores, queries], axis=1),
            jnp.concatenate([scaled, entering], axis=0),
            preferred_element_type=F32,
        )
        y_ref[:, lanes] = mixed * from_middle[:, lanes]
        gained = lax.dot_general(
            keys, scaled, (((0,), (0,)), ((), ())), preferred_element_type=F32
        )
        carried[group] = state * at_end[:, lanes] + gained * middle_to_end[:, lanes]

    @pl.when(turn == pl.num_programs(0) - 1)
    def _():
        whole = spread(jnp.exp(before[...]), table)
        wide = (groups // 2) * STATE_WIDE
        last = state_ref.shape[0] - FADE_ROWS
        row = lax.broadcasted_iota(jnp.int32, (FADE_ROWS, GROUP_COLS), 0)
        fades = jnp.zeros((FADE_ROWS, GROUP_COLS), F32)
        for group in range(groups):
            place = group // 2
            lanes = slice(group * GROUP_COLS, (group + 1) * GROUP_COLS)
            fades = jnp.where(row == group, whole[0:1, lanes], fades)
            if group % 2 == 0:
                at = place * STATE_WIDE
                state_ref[at : at + STATE_WIDE, :] = carried[group].astype(BF16)
            else:
                inner = (place % 2) * STATE_NARROW
                at = wide + place * STATE_NARROW
                state_ref[at : at + STATE_NARROW, :] = carried[group][
                    inner : inner + STATE_NARROW, :
                ].astype(BF16)
        state_ref[last:, :] = fades.astype(BF16)


def joined(later, earlier):
    last = later.shape[0] - FADE_ROWS
    groups = last // (STATE_WIDE + STATE_NARROW) * 2
    wide = (groups // 2) * STATE_WIDE
    later, earlier = later.astype(F32), earlier.astype(F32)
    parts = []
    for place in range(groups // 2):
        rows = slice(place * STATE_WIDE, (place + 1) * STATE_WIDE)
        fade = later[last + 2 * place : last + 2 * place + 1]
        parts.append(fade * earlier[rows] + later[rows])
    for place in range(groups // 2):
        rows = slice(wide + place * STATE_NARROW, wide + (place + 1) * STATE_NARROW)
        fade = later[last + 2 * place + 1 : last + 2 * place + 2]
        parts.append(fade * earlier[rows] + later[rows])
    parts.append(later[last:] * earlier[last:])
    return jnp.concatenate(parts, axis=0).astype(BF16)


def join_body(later_ref, earlier_ref, out_ref):
    out_ref[...] = joined(later_ref[...], earlier_ref[...])


def join_call(later, earlier):
    return pl.pallas_call(
        join_body,
        out_shape=jax.ShapeDtypeStruct(later.shape, BF16),
        compiler_params=pltpu.CompilerParams(vmem_limit_bytes=VMEM_LIMIT),
        name="join_states",
    )(later, earlier)


def final_body(
    ids_ref, y_ref, q_ref, fade_ref, gate_ref, gain_ref, near_ref, far_ref, matrix_ref, *rest
):
    out_refs, (state, normed, matrix, arrived) = rest[:-4], rest[-4:]
    rows, columns = y_ref.shape
    heads = fade_ref.shape[1]
    table = head_table(heads, columns)
    turn = pl.program_id(0)
    copy = pltpu.make_async_copy(matrix_ref, matrix, arrived)

    @pl.when(turn == 0)
    def _():
        copy.start()
        state[...] = joined(near_ref[...], far_ref[...])

    fade = spread(fade_ref[...], table)
    groups = columns // GROUP_COLS
    wide = (groups // 2) * STATE_WIDE
    parts = []
    squares = []
    for group in range(groups):
        place = group // 2
        lanes = slice(group * GROUP_COLS, (group + 1) * GROUP_COLS)
        if group % 2 == 0:
            at = place * STATE_WIDE
            queries = q_ref[:, at : at + STATE_WIDE]
        else:
            at = wide + (place // 2) * STATE_WIDE
            queries = q_ref[:, at : at + STATE_WIDE]
            queries = jnp.where(
                narrow_mask(place % 2, rows, STATE_WIDE), queries, jnp.zeros_like(queries)
            )
        outer = jnp.dot(queries, state[at : at + STATE_WIDE, :], preferred_element_type=F32)
        mixed = y_ref[:, lanes] + outer * fade[:, lanes]
        gated = mixed * silu(gate_ref[:, lanes].astype(F32))
        parts.append(gated)
        square = (gated * gated).astype(BF16)
        squares.append(
            lax.dot_general(
                square,
                table[0:heads, lanes],
                (((1,), (1,)), ((), ())),
                preferred_element_type=F32,
            )
        )
    mean = functools.reduce(jnp.add, squares) * (1.0 / HEAD_DIM)
    scale = spread(lax.rsqrt(mean + 1e-06), table)
    at = pl.multiple_of(turn * rows, rows)
    for group in range(groups):
        lanes = slice(group * GROUP_COLS, (group + 1) * GROUP_COLS)
        gain = gain_ref[0:1, lanes].astype(F32)
        normed[pl.ds(at, rows), lanes] = (parts[group] * scale[:, lanes] * gain).astype(BF16)

    @pl.when(turn == pl.num_programs(0) - 1)
    def _():
        copy.wait()
        step = 512
        for start in range(0, matrix.shape[1], step):
            product = jnp.dot(
                normed[...], matrix[:, start : start + step], preferred_element_type=F32
            )
            at = 0
            for out_ref in out_refs:
                size = out_ref.shape[0]
                out_ref[:, start : start + step] = product[at : at + size].astype(out_ref.dtype)
                at += size


def local_call(raw, step, extra, rate, rim, taps):
    length, columns = raw[0].shape
    heads = step.shape[0]
    chunk = CHUNK
    groups = columns // GROUP_COLS
    width = rim.shape[1]
    states = raw[1].shape[1] + raw[3].shape[1]

    def rows(array):
        return pl.BlockSpec((chunk, array.shape[1]), lambda i: (i, 0))

    def fixed(shape):
        return pl.BlockSpec(shape, lambda i: tuple(0 for _ in shape))

    turned = pl.BlockSpec((heads, chunk), lambda i: (0, i))
    return pl.pallas_call(
        local_body,
        grid=(length // chunk,),
        in_specs=[rows(a) for a in raw]
        + [turned, turned, fixed(rate.shape), fixed(rim.shape)]
        + [fixed(t.shape) for t in taps],
        out_specs=[
            pl.BlockSpec((chunk, columns), lambda i: (i, 0)),
            pl.BlockSpec((chunk, states), lambda i: (i, 0)),
            pl.BlockSpec((chunk, heads), lambda i: (i, 0)),
            fixed((states + FADE_ROWS, GROUP_COLS)),
        ],
        out_shape=[
            jax.ShapeDtypeStruct((length, columns), F32),
            jax.ShapeDtypeStruct((length, states), BF16),
            jax.ShapeDtypeStruct((length, heads), F32),
            jax.ShapeDtypeStruct((states + FADE_ROWS, GROUP_COLS), BF16),
        ],
        scratch_shapes=[
            pltpu.VMEM((8 + chunk, width), F32),
            pltpu.VMEM((groups, STATE_WIDE, GROUP_COLS), F32),
            pltpu.VMEM((8, heads), F32),
        ],
        compiler_params=pltpu.CompilerParams(dimension_semantics=("arbitrary",)),
        cost_estimate=pl.CostEstimate(
            flops=12_000_000_000, bytes_accessed=10_000_000, transcendentals=0
        ),
        name="mix_local",
    )(*raw, step, extra, rate, rim, *taps)


def final_call(ids, y, q, fade, gate, gain, near, far, matrix, rows_each, outs):
    columns = y.shape[1]
    width = matrix.shape[1]
    count = ids.shape[0]

    def rows(array):
        return pl.BlockSpec((rows_each, array.shape[1]), lambda i, ids: (ids[i], 0))

    def fixed(array):
        return pl.BlockSpec(array.shape, lambda i, ids: (0, 0))

    return pl.pallas_call(
        final_body,
        grid_spec=pltpu.PrefetchScalarGridSpec(
            num_scalar_prefetch=1,
            grid=(count,),
            in_specs=[rows(y), rows(q), rows(fade), rows(gate)]
            + [fixed(a) for a in (gain, near, far)]
            + [pl.BlockSpec(memory_space=pl.ANY)],
            out_specs=[
                pl.BlockSpec((n * rows_each, width), lambda i, ids: (0, 0)) for n, _ in outs
            ],
            scratch_shapes=[
                pltpu.VMEM(near.shape, BF16),
                pltpu.VMEM((rows_each * count, columns), BF16),
                pltpu.VMEM(matrix.shape, BF16),
                pltpu.SemaphoreType.DMA,
            ],
        ),
        out_shape=[jax.ShapeDtypeStruct((n * rows_each, width), kind) for n, kind in outs],
        compiler_params=pltpu.CompilerParams(vmem_limit_bytes=VMEM_LIMIT),
        cost_estimate=pl.CostEstimate(
            flops=6_000_000_000, bytes_accessed=10_000_000, transcendentals=0
        ),
        name="mix_final",
    )(ids, y, q, fade, gate, gain, near, far, matrix)


def settle_body(residual_ref, kept_ref, near_ref, far_ref, gain_ref, after_ref, norm_ref):
    total = kept_ref[...] + near_ref[...].astype(F32) + far_ref[...].astype(F32)
    after = (residual_ref[...].astype(F32) + total).astype(BF16)
    after_ref[...] = after
    wide = after.astype(F32)
    mean = jnp.mean(wide * wide, axis=-1, keepdims=True)
    norm_ref[...] = (wide * lax.rsqrt(mean + 1e-06) * gain_ref[...].astype(F32)).astype(BF16)


def settle_call(residual, kept, near, far, gain):
    rows, width = residual.shape
    top = pl.BlockSpec((rows // 2, width), lambda i: (i, 0))
    return pl.pallas_call(
        settle_body,
        grid=(2,),
        in_specs=[top] * 4 + [pl.BlockSpec(gain.shape, lambda i: (0, 0))],
        out_specs=[top, top],
        out_shape=[jax.ShapeDtypeStruct(residual.shape, BF16)] * 2,
        compiler_params=pltpu.CompilerParams(vmem_limit_bytes=VMEM_LIMIT),
        name="settle",
    )(residual, kept, near, far, gain)


def finish_body(after_ref, kept_ref, came_ref, l1_ref, l2_ref, r1_ref, r2_ref, out_ref):
    half = l1_ref.shape[1]
    share = kept_ref[...].astype(F32) + came_ref[...].astype(F32)
    left = share[:, :half] + l1_ref[...].astype(F32) + l2_ref[...].astype(F32)
    right = share[:, half:] + r1_ref[...].astype(F32) + r2_ref[...].astype(F32)
    out_ref[:, :half] = (after_ref[:, :half].astype(F32) + 0.5 * left).astype(BF16)
    out_ref[:, half:] = (after_ref[:, half:].astype(F32) + 0.5 * right).astype(BF16)


def finish_call(*arrays):
    rows, width = arrays[0].shape
    each = rows // 2
    return pl.pallas_call(
        finish_body,
        grid=(2,),
        in_specs=[pl.BlockSpec((each, a.shape[1]), lambda i: (i, 0)) for a in arrays],
        out_specs=pl.BlockSpec((each, width), lambda i: (i, 0)),
        out_shape=jax.ShapeDtypeStruct((rows, width), BF16),
        compiler_params=pltpu.CompilerParams(vmem_limit_bytes=VMEM_LIMIT),
        name="finish",
    )(*arrays)


def pick_body(part_ref, gate_ref, up_ref, down_ref, out_ref):
    columns = gate_ref.shape[1]
    for k, ref in enumerate((gate_ref, up_ref, down_ref)):
        out_ref[:, k * columns : (k + 1) * columns] = ref[...]


def pick_call(part, parts, weights):
    rows, columns = weights[0].shape
    columns //= parts
    return pl.pallas_call(
        pick_body,
        grid_spec=pltpu.PrefetchScalarGridSpec(
            num_scalar_prefetch=1,
            grid=(1,),
            in_specs=[pl.BlockSpec((rows, columns), lambda i, part: (0, part[0]))] * 3,
            out_specs=pl.BlockSpec((rows, 3 * columns), lambda i, part: (0, 0)),
        ),
        out_shape=jax.ShapeDtypeStruct((rows, 3 * columns), BF16),
        name="pick",
    )(part, *weights)


def feed_body(place_ref, *refs, pieces):
    own_ref, moved = refs[0], refs[1 : 2 * pieces - 1]
    x_refs = refs[2 * pieces - 1 : -4]
    out_refs, weights, arrived = refs[-4:-2], refs[-2], refs[-1]
    place, odd = place_ref[0], place_ref[1]
    copies = [pltpu.make_async_copy(own_ref, weights.at[0], arrived.at[0])]
    copies[0].start()
    for k in range(1, pieces):
        target = weights.at[k], arrived.at[k]
        copies.append(pltpu.make_async_copy(own_ref, *target))
        for ahead in (True, False):
            steps = k if ahead else pieces - k
            stream, back = moved[2 * steps - 2 : 2 * steps]
            side = place + k < pieces if ahead else place + k >= pieces

            @pl.when(side & (odd == int(ahead)))
            def _(stream=stream, target=target):
                source = stream if len(stream.shape) == 2 else stream.at[0]
                pltpu.make_async_copy(source, *target).start()

            @pl.when(side & (odd != int(ahead)))
            def _(back=back, target=target):
                pltpu.make_async_copy(back, *target).start()

    depth = weights.shape[1]
    columns = weights.shape[2] // 3
    rows = out_refs[0].shape[0]

    def run(k):
        at = lax.rem(place_ref[0] + k, pieces) if pieces > 1 else 0
        return pl.ds(pl.multiple_of(at * depth, depth), depth)

    total = None
    for k, copy in enumerate(copies):
        copy.wait()
        x = jnp.concatenate([x_ref[:, run(k)] for x_ref in x_refs], axis=0)
        term = jnp.dot(x, weights[k, :, : 2 * columns], preferred_element_type=F32)
        total = term if total is None else total + term
    hidden = (silu(total[:, :columns]) * total[:, columns:]).astype(BF16)
    for k in range(pieces):
        product = lax.dot_general(
            hidden,
            weights[k, :, 2 * columns :],
            (((1,), (1,)), ((), ())),
            preferred_element_type=F32,
        ).astype(BF16)
        out_refs[0][:, run(k)] = product[:rows]
        out_refs[1][:, run(k)] = product[rows:]


def feed_call(place, kept, away, weights):
    width = kept[0].shape[1]
    pieces = (len(weights) + 1) // 2
    columns = weights[0].shape[1] // 3
    rows = sum(a.shape[0] for a in kept)
    outs = jax.ShapeDtypeStruct((rows, width), BF16)
    whole = pl.BlockSpec(memory_space=pltpu.VMEM)
    return pl.pallas_call(
        functools.partial(feed_body, pieces=pieces),
        in_specs=[pl.BlockSpec(memory_space=pltpu.SMEM)]
        + [pl.BlockSpec(memory_space=pltpu.HBM)] * len(weights)
        + [whole] * (len(kept) + len(away)),
        out_specs=[whole, whole],
        out_shape=[outs, outs],
        scratch_shapes=[
            pltpu.VMEM((pieces, *weights[0].shape), BF16),
            pltpu.SemaphoreType.DMA((pieces,)),
        ],
        cost_estimate=pl.CostEstimate(
            flops=12 * rows * width * columns, bytes_accessed=8_000_000, transcendentals=0
        ),
        compiler_params=pltpu.CompilerParams(vmem_limit_bytes=VMEM_LIMIT),
        name="feed",
    )(place, *weights, *kept, *away)


def halves(ref, came):
    both = ref.astype(F32) + came.astype(F32)
    half = both.shape[1] // 2
    return both[:, :half].astype(BF16), both[:, half:].astype(BF16)


def feed_forward(x_norm, after_mixer, weights):
    rows, _ = x_norm.shape
    half = rows // 2
    spot = jnp.stack([lax.axis_index("sp"), lax.axis_index("tp") & 1])

    x1 = x_norm
    x_side = swapped(x1, "tp", 2)
    y_side = swapped(x1, "grp", 1)
    x1_away = swapped(x1, "tp", 1)
    corner_top = swapped(y_side[:half], "tp", 2)
    corner_low = swapped(x_side[half:], "grp", 1)
    x_away = swapped(x_side, "tp", 1)
    y_away = swapped(y_side, "tp", 1)
    top_away = swapped(corner_top, "tp", 1)
    low_away = swapped(corner_low, "tp", 1)

    def feed(kept, away):
        mine, theirs = feed_call(spot, kept, away, weights)
        return mine, swapped(theirs, "tp", 1)

    own, own_came = feed([x1], [x1_away])
    xs, xs_came = feed([x_side], [x_away])
    corner, corner_came = feed([corner_top, corner_low], [top_away, low_away])
    ys, ys_came = feed([y_side], [y_away])
    x_left, x_right = halves(xs, xs_came)
    y_left, y_right = halves(ys, ys_came)
    l1 = swapped(x_left, "tp", 2)
    r1 = swapped(y_right, "grp", 1)
    c_left, c_right = halves(corner, corner_came)
    l2 = swapped(c_left, "tp", 2)
    r2 = swapped(c_right, "grp", 1)
    y_left = (y_left.astype(F32) + l2.astype(F32)).astype(BF16)
    x_right = (x_right.astype(F32) + r2.astype(F32)).astype(BF16)
    l2 = swapped(y_left, "grp", 1)
    r2 = swapped(x_right, "tp", 2)
    return finish_call(after_mixer, own, own_came, l1, l2, r1, r2)


def feed_forward_any(x_norm, after_mixer, weights):
    (weight,) = weights
    columns = weight.shape[1] // 3
    x = lax.all_gather(x_norm, ("grp", "tp"), axis=0, tiled=True)
    gates = jnp.dot(x, weight[:, :columns], preferred_element_type=F32)
    ups = jnp.dot(x, weight[:, columns : 2 * columns], preferred_element_type=F32)
    hidden = (silu(gates) * ups).astype(BF16)
    share = lax.dot_general(
        hidden,
        weight[:, 2 * columns :],
        (((1,), (1,)), ((), ())),
        preferred_element_type=F32,
    ).astype(BF16)
    share = lax.psum_scatter(share, ("grp", "tp"), scatter_dimension=0, tiled=True)
    return (after_mixer.astype(F32) + 0.5 * share.astype(F32)).astype(BF16)


def shifted(value, axis, steps):
    count = lax.axis_size(axis)
    return lax.ppermute(value, axis, [(s, s + steps) for s in range(count - steps)])


def either_way(value):
    count, members = lax.axis_size("sp"), lax.axis_size("tp")
    pairs = []
    for s in range(count):
        for t in range(members):
            target = s - 1 if t % 2 else s + 1
            if 0 <= target < count:
                pairs.append((s * members + t, target * members + t))
    return lax.ppermute(value, ("sp", "tp"), pairs)


def swapped(value, axis, bit):
    count = lax.axis_size(axis)
    return lax.ppermute(value, axis, [(s, s ^ bit) for s in range(count)])


def entering_states(packed, axis):
    count = lax.axis_size(axis)
    window, before, got = packed, None, jnp.zeros_like(packed)
    reach = 1
    while reach < count:
        if reach > 1:
            window = join_call(window, got)
            before = got if before is None else join_call(before, got)
        got = shifted(window, axis, reach)
        reach *= 2
    return (got, jnp.zeros_like(got)) if before is None else (before, got)


def on_device(
    residual,
    value_projected,
    gate_projected,
    wide_key_rows,
    wide_query_rows,
    narrow_key_rows,
    narrow_query_rows,
    step_before_softplus,
    extra_log_decay,
    log_decay_rate,
    value_kernel,
    wide_key_kernel,
    wide_query_kernel,
    narrow_key_kernel,
    narrow_query_kernel,
    head_norm_gain,
    output_matrix,
    feedforward_norm_gain,
    gate_matrix,
    up_matrix,
    down_matrix,
):
    members = lax.axis_size("tp")
    place = lax.axis_index("tp")
    part = jnp.reshape(lax.axis_index("grp"), (1,))
    mine = pick_call(part, lax.axis_size("grp"), (gate_matrix, up_matrix, down_matrix))
    raw = (value_projected, wide_key_rows, wide_query_rows, narrow_key_rows, narrow_query_rows)
    rim = shifted(tails_call(raw), "sp", 1)
    count = lax.axis_size("sp")
    direct = members == 4 and lax.axis_size("grp") == 2 and count == 4
    if direct:
        mine, rim = lax.optimization_barrier((mine, rim))
        first = either_way(mine)
    else:
        weights = [lax.all_gather(mine, "sp", axis=0, tiled=True)]

    taps = (
        value_kernel,
        wide_key_kernel,
        wide_query_kernel,
        narrow_key_kernel,
        narrow_query_kernel,
    )
    y, q, fade, packed = local_call(
        raw, step_before_softplus.T, extra_log_decay.T, log_decay_rate[None, :], rim, taps
    )
    if direct:
        mine, packed = lax.optimization_barrier((mine, packed))
    near, far = entering_states(packed, "sp")
    if direct:
        pair = jnp.stack([first, swapped(mine, "tp", 1)])
    if direct:
        pair, near, far = lax.optimization_barrier((pair, near, far))
        streams = [first]
        backs = []
        for k in range(2, count + 1):
            pair = either_way(pair if k < count else pair[1])
            if k < count:
                streams.append(pair)
            backs.append(swapped(pair[1] if k < count else pair, "tp", 1))
        weights = [mine]
        for stream, back in zip(streams, backs):
            weights += [stream, back]

    rows = y.shape[0] // members
    masks = 2 * jnp.arange(members // 2, dtype=jnp.int32)
    shared = (y, q, fade, gate_projected, head_norm_gain[None, :], near, far, output_matrix, rows)
    half = members // 2
    ids = jnp.concatenate([(place ^ 1) ^ masks, place ^ masks[1:]])
    away, far_kept = final_call(ids, *shared, [(half, BF16), (half - 1, BF16)])
    came = swapped(away, "tp", 1)
    (kept,) = final_call(place ^ masks[:1], *shared, [(1, F32)])
    bit = members // 2
    total = {}

    def block(array, index):
        return array[index * rows : (index + 1) * rows]

    for mask in range(2, members, 2):
        total[mask] = block(far_kept, mask // 2 - 1).astype(F32) + block(came, mask // 2).astype(F32)
    last = None
    while bit > 1:
        for mask in range(0, bit, 2):
            got = swapped(total[mask + bit].astype(BF16), "tp", bit)
            if mask == 0:
                last = got if last is None else last.astype(F32) + got.astype(F32)
            else:
                total[mask] = total[mask] + got.astype(F32)
        bit //= 2
    after_mixer, x_norm = settle_call(residual, kept, came, last, feedforward_norm_gain[None, :])
    if members == 4 and lax.axis_size("grp") == 2:
        return feed_forward(x_norm, after_mixer, weights)
    return feed_forward_any(x_norm, after_mixer, weights)


def solution(mesh):
    in_specs = (
        P(("grp", "sp", "tp"), None),
        P(("grp", "sp"), "tp"),
        P(("grp", "sp"), "tp"),
        P(("grp", "sp"), "tp"),
        P(("grp", "sp"), "tp"),
        P(("grp", "sp"), "tp"),
        P(("grp", "sp"), "tp"),
        P(("grp", "sp"), "tp"),
        P(("grp", "sp"), "tp"),
        P("tp"),
        P(None, "tp"),
        P(None, "tp"),
        P(None, "tp"),
        P(None, "tp"),
        P(None, "tp"),
        P("tp"),
        P("tp", None),
        P(),
        P("sp", "tp"),
        P("sp", "tp"),
        P("sp", "tp"),
    )
    out_specs = P(("grp", "sp", "tp"), None)

    return jax.shard_map(
        on_device, mesh=mesh, in_specs=in_specs, out_specs=out_specs, check_vma=False
    )
```

```python
import functools
import jax
import jax.numpy as jnp
from jax import lax
from jax.experimental import pallas as pl
from jax.experimental.pallas import tpu as pltpu
from jax.sharding import PartitionSpec as P


HEAD_DIM = 64
PER_GROUP = 4
GROUP_COLS = HEAD_DIM * PER_GROUP
STATE_WIDE = 128
STATE_NARROW = 64
CHUNK = 128
TAIL = 16
FADE_ROWS = 16
VMEM_LIMIT = 16 * 1024 * 1024
F32 = jnp.float32
BF16 = jnp.bfloat16


def silu(x):
    half = 0.5 * x
    return half + half * jnp.tanh(half)


def spread(values, table):
    high = values.astype(BF16).astype(F32)
    low = values - high
    return jnp.dot(
        jnp.concatenate([high, low], axis=1).astype(BF16), table, preferred_element_type=F32
    )


def head_table(heads, columns):
    head = lax.broadcasted_iota(jnp.int32, (2 * heads, columns), 0)
    head = jnp.where(head >= heads, head - heads, head)
    column = lax.broadcasted_iota(jnp.int32, (2 * heads, columns), 1)
    inside = (column >= head * HEAD_DIM) & (column < (head + 1) * HEAD_DIM)
    return jnp.where(inside, 1.0, 0.0).astype(BF16)


def narrow_mask(place, rows, lanes):
    lane = lax.broadcasted_iota(jnp.int32, (rows, lanes), 1)
    start = place * STATE_NARROW
    return (lane >= start) & (lane < start + STATE_NARROW)


def tails_body(*refs):
    out_ref, arrived = refs[-2:]
    copies = []
    offset = 0
    for k, ref in enumerate(refs[:-2]):
        rows, columns = ref.shape
        copies.append(
            pltpu.make_async_copy(
                ref.at[rows - TAIL :, :], out_ref.at[:, offset : offset + columns], arrived.at[k]
            )
        )
        offset += columns
    for copy in copies:
        copy.start()
    for copy in copies:
        copy.wait()


def tails_call(raw):
    width = sum(a.shape[1] for a in raw)
    return pl.pallas_call(
        tails_body,
        in_specs=[pl.BlockSpec(memory_space=pltpu.HBM)] * len(raw),
        out_specs=pl.BlockSpec(memory_space=pltpu.VMEM),
        out_shape=jax.ShapeDtypeStruct((TAIL, width), BF16),
        scratch_shapes=[pltpu.SemaphoreType.DMA((len(raw),))],
        name="tails",
    )(*raw)


def local_body(
    value_ref,
    kw_ref,
    qw_ref,
    kn_ref,
    qn_ref,
    step_ref,
    extra_ref,
    rate_ref,
    rim_ref,
    value_taps,
    kw_taps,
    qw_taps,
    kn_taps,
    qn_taps,
    y_ref,
    q_ref,
    fade_ref,
    state_ref,
    raw,
    carried,
    before,
):
    turn = pl.program_id(0)
    chunk = value_ref.shape[0]
    heads = step_ref.shape[0]
    columns = value_ref.shape[1]
    table = head_table(heads, columns)

    @pl.when(turn == 0)
    def _():
        raw[0:8, :] = rim_ref[...].astype(F32)[TAIL - 8 :, :]
        carried[...] = jnp.zeros_like(carried)
        before[...] = jnp.zeros_like(before)

    @pl.when(turn > 0)
    def _():
        raw[0:8, :] = raw[chunk : chunk + 8, :]

    starts = []
    offset = 0
    for ref in (value_ref, kw_ref, qw_ref, kn_ref, qn_ref):
        starts.append(offset)
        raw[8 : 8 + chunk, offset : offset + ref.shape[1]] = ref[...].astype(F32)
        offset += ref.shape[1]

    def conv(which, start, width):
        taps_ref = (value_taps, kw_taps, qw_taps, kn_taps, qn_taps)[which]
        weights = taps_ref[:, start : start + width].astype(F32)
        taps = weights.shape[0]
        start = starts[which] + start
        total = None
        for tap in range(taps):
            first = 8 - (taps - 1) + tap
            term = raw[first : first + chunk, start : start + width] * weights[tap : tap + 1]
            total = term if total is None else total + term
        return silu(total).astype(BF16)

    step = jnp.log(1.0 + jnp.exp(step_ref[...].T))
    decay = extra_ref[...].T - jnp.exp(rate_ref[...]) * step
    row = lax.broadcasted_iota(jnp.int32, (chunk, chunk), 0)
    column = lax.broadcasted_iota(jnp.int32, (chunk, chunk), 1)
    lower = row >= column
    first = decay.astype(BF16).astype(F32)
    second = (decay - first).astype(BF16).astype(F32)
    terms = jnp.concatenate([first, second, decay - first - second], axis=1).astype(BF16)
    sums = jnp.dot(
        jnp.where(lower, 1.0, 0.0).astype(BF16), terms, preferred_element_type=F32
    )
    running = sums[:, :heads] + sums[:, heads : 2 * heads] + sums[:, 2 * heads :]
    middle = running[chunk // 2 - 1 : chunk // 2, :]
    total = running[chunk - 1 : chunk, :]
    since = jnp.exp(running)
    fade_ref[...] = jnp.exp(running + before[0:1, :])
    before[...] = before[...] + total
    factors = spread(
        jnp.concatenate(
            [
                jnp.exp(middle - running) * step,
                jnp.exp(running - middle),
                since[chunk // 2 - 8 : chunk // 2],
                since[chunk - 8 : chunk],
            ],
            axis=0,
        ),
        table,
    )
    to_middle = factors[:chunk]
    from_middle = factors[chunk : 2 * chunk]
    at_middle = factors[2 * chunk + 7 : 2 * chunk + 8, :]
    at_end = factors[2 * chunk + 15 : 2 * chunk + 16, :]
    middle_to_end = from_middle[chunk - 1 : chunk, :]

    groups = columns // GROUP_COLS
    for group in range(groups):
        place = group // 2
        lanes = slice(group * GROUP_COLS, (group + 1) * GROUP_COLS)
        values = conv(0, group * GROUP_COLS, GROUP_COLS)
        scaled = (values.astype(F32) * to_middle[:, lanes]).astype(BF16)
        if group % 2 == 0:
            keys = conv(1, place * STATE_WIDE, STATE_WIDE)
            queries = conv(2, place * STATE_WIDE, STATE_WIDE)
            q_ref[:, place * STATE_WIDE : (place + 1) * STATE_WIDE] = queries
        else:
            pair = place // 2
            inner = place % 2
            if inner == 0:
                keys_n = conv(3, pair * STATE_WIDE, STATE_WIDE)
                queries_n = conv(4, pair * STATE_WIDE, STATE_WIDE)
                first = kw_ref.shape[1] + pair * STATE_WIDE
                q_ref[:, first : first + STATE_WIDE] = queries_n
            mask = narrow_mask(inner, chunk, STATE_WIDE)
            keys = jnp.where(mask, keys_n, jnp.zeros_like(keys_n))
            queries = queries_n
        scores = lax.dot_general(
            queries, keys, (((1,), (1,)), ((), ())), preferred_element_type=F32
        )
        scores = jnp.where(lower, scores, 0.0).astype(BF16)
        state = carried[group]
        entering = (state * at_middle[:, lanes]).astype(BF16)
        mixed = jnp.dot(
            jnp.concatenate([scores, queries], axis=1),
            jnp.concatenate([scaled, entering], axis=0),
            preferred_element_type=F32,
        )
        y_ref[:, lanes] = (mixed * from_middle[:, lanes]).astype(BF16)
        gained = lax.dot_general(
            keys, scaled, (((0,), (0,)), ((), ())), preferred_element_type=F32
        )
        carried[group] = state * at_end[:, lanes] + gained * middle_to_end[:, lanes]

    @pl.when(turn == pl.num_programs(0) - 1)
    def _():
        whole = spread(jnp.exp(before[...]), table)
        wide = (groups // 2) * STATE_WIDE
        last = state_ref.shape[0] - FADE_ROWS
        row = lax.broadcasted_iota(jnp.int32, (FADE_ROWS, GROUP_COLS), 0)
        fades = jnp.zeros((FADE_ROWS, GROUP_COLS), F32)
        for group in range(groups):
            place = group // 2
            lanes = slice(group * GROUP_COLS, (group + 1) * GROUP_COLS)
            fades = jnp.where(row == group, whole[0:1, lanes], fades)
            if group % 2 == 0:
                at = place * STATE_WIDE
                state_ref[at : at + STATE_WIDE, :] = carried[group].astype(BF16)
            else:
                inner = (place % 2) * STATE_NARROW
                at = wide + place * STATE_NARROW
                state_ref[at : at + STATE_NARROW, :] = carried[group][
                    inner : inner + STATE_NARROW, :
                ].astype(BF16)
        state_ref[last:, :] = fades.astype(BF16)


def joined(later, earlier):
    last = later.shape[0] - FADE_ROWS
    groups = last // (STATE_WIDE + STATE_NARROW) * 2
    wide = (groups // 2) * STATE_WIDE
    later, earlier = later.astype(F32), earlier.astype(F32)
    parts = []
    for place in range(groups // 2):
        rows = slice(place * STATE_WIDE, (place + 1) * STATE_WIDE)
        fade = later[last + 2 * place : last + 2 * place + 1]
        parts.append(fade * earlier[rows] + later[rows])
    for place in range(groups // 2):
        rows = slice(wide + place * STATE_NARROW, wide + (place + 1) * STATE_NARROW)
        fade = later[last + 2 * place + 1 : last + 2 * place + 2]
        parts.append(fade * earlier[rows] + later[rows])
    parts.append(later[last:] * earlier[last:])
    return jnp.concatenate(parts, axis=0).astype(BF16)


def join_body(later_ref, earlier_ref, out_ref):
    out_ref[...] = joined(later_ref[...], earlier_ref[...])


def join_call(later, earlier):
    return pl.pallas_call(
        join_body,
        out_shape=jax.ShapeDtypeStruct(later.shape, BF16),
        compiler_params=pltpu.CompilerParams(vmem_limit_bytes=VMEM_LIMIT),
        name="join_states",
    )(later, earlier)


def final_body(
    ids_ref, y_ref, q_ref, fade_ref, gate_ref, gain_ref, near_ref, far_ref, matrix_ref, *rest
):
    out_refs, (state, normed, matrix, arrived) = rest[:-4], rest[-4:]
    rows, columns = y_ref.shape
    heads = fade_ref.shape[1]
    table = head_table(heads, columns)
    turn = pl.program_id(0)
    copy = pltpu.make_async_copy(matrix_ref, matrix, arrived)

    @pl.when(turn == 0)
    def _():
        copy.start()
        state[...] = joined(near_ref[...], far_ref[...])

    fade = spread(fade_ref[...], table)
    groups = columns // GROUP_COLS
    wide = (groups // 2) * STATE_WIDE
    parts = []
    squares = []
    for group in range(groups):
        place = group // 2
        lanes = slice(group * GROUP_COLS, (group + 1) * GROUP_COLS)
        if group % 2 == 0:
            at = place * STATE_WIDE
            queries = q_ref[:, at : at + STATE_WIDE]
        else:
            at = wide + (place // 2) * STATE_WIDE
            queries = q_ref[:, at : at + STATE_WIDE]
            queries = jnp.where(
                narrow_mask(place % 2, rows, STATE_WIDE), queries, jnp.zeros_like(queries)
            )
        outer = jnp.dot(queries, state[at : at + STATE_WIDE, :], preferred_element_type=F32)
        mixed = y_ref[:, lanes].astype(F32) + outer * fade[:, lanes]
        gated = mixed * silu(gate_ref[:, lanes].astype(F32))
        parts.append(gated)
        square = (gated * gated).astype(BF16)
        squares.append(
            lax.dot_general(
                square,
                table[0:heads, lanes],
                (((1,), (1,)), ((), ())),
                preferred_element_type=F32,
            )
        )
    mean = functools.reduce(jnp.add, squares) * (1.0 / HEAD_DIM)
    scale = spread(lax.rsqrt(mean + 1e-06), table)
    at = pl.multiple_of(turn * rows, rows)
    for group in range(groups):
        lanes = slice(group * GROUP_COLS, (group + 1) * GROUP_COLS)
        gain = gain_ref[0:1, lanes].astype(F32)
        normed[pl.ds(at, rows), lanes] = (parts[group] * scale[:, lanes] * gain).astype(BF16)

    @pl.when(turn == pl.num_programs(0) - 1)
    def _():
        copy.wait()
        step = 512
        for start in range(0, matrix.shape[1], step):
            product = jnp.dot(
                normed[...], matrix[:, start : start + step], preferred_element_type=F32
            )
            at = 0
            for out_ref in out_refs:
                size = out_ref.shape[0]
                out_ref[:, start : start + step] = product[at : at + size].astype(out_ref.dtype)
                at += size


def local_call(raw, step, extra, rate, rim, taps):
    length, columns = raw[0].shape
    heads = step.shape[0]
    chunk = CHUNK
    groups = columns // GROUP_COLS
    width = rim.shape[1]
    states = raw[1].shape[1] + raw[3].shape[1]

    def rows(array):
        return pl.BlockSpec((chunk, array.shape[1]), lambda i: (i, 0))

    def fixed(shape):
        return pl.BlockSpec(shape, lambda i: tuple(0 for _ in shape))

    turned = pl.BlockSpec((heads, chunk), lambda i: (0, i))
    return pl.pallas_call(
        local_body,
        grid=(length // chunk,),
        in_specs=[rows(a) for a in raw]
        + [turned, turned, fixed(rate.shape), fixed(rim.shape)]
        + [fixed(t.shape) for t in taps],
        out_specs=[
            pl.BlockSpec((chunk, columns), lambda i: (i, 0)),
            pl.BlockSpec((chunk, states), lambda i: (i, 0)),
            pl.BlockSpec((chunk, heads), lambda i: (i, 0)),
            fixed((states + FADE_ROWS, GROUP_COLS)),
        ],
        out_shape=[
            jax.ShapeDtypeStruct((length, columns), BF16),
            jax.ShapeDtypeStruct((length, states), BF16),
            jax.ShapeDtypeStruct((length, heads), F32),
            jax.ShapeDtypeStruct((states + FADE_ROWS, GROUP_COLS), BF16),
        ],
        scratch_shapes=[
            pltpu.VMEM((8 + chunk, width), F32),
            pltpu.VMEM((groups, STATE_WIDE, GROUP_COLS), F32),
            pltpu.VMEM((8, heads), F32),
        ],
        compiler_params=pltpu.CompilerParams(dimension_semantics=("arbitrary",)),
        cost_estimate=pl.CostEstimate(
            flops=12_000_000_000, bytes_accessed=10_000_000, transcendentals=0
        ),
        name="mix_local",
    )(*raw, step, extra, rate, rim, *taps)


def final_call(ids, y, q, fade, gate, gain, near, far, matrix, rows_each, outs):
    columns = y.shape[1]
    width = matrix.shape[1]
    count = ids.shape[0]

    def rows(array):
        return pl.BlockSpec((rows_each, array.shape[1]), lambda i, ids: (ids[i], 0))

    def fixed(array):
        return pl.BlockSpec(array.shape, lambda i, ids: (0, 0))

    return pl.pallas_call(
        final_body,
        grid_spec=pltpu.PrefetchScalarGridSpec(
            num_scalar_prefetch=1,
            grid=(count,),
            in_specs=[rows(y), rows(q), rows(fade), rows(gate)]
            + [fixed(a) for a in (gain, near, far)]
            + [pl.BlockSpec(memory_space=pl.ANY)],
            out_specs=[
                pl.BlockSpec((n * rows_each, width), lambda i, ids: (0, 0)) for n, _ in outs
            ],
            scratch_shapes=[
                pltpu.VMEM(near.shape, BF16),
                pltpu.VMEM((rows_each * count, columns), BF16),
                pltpu.VMEM(matrix.shape, BF16),
                pltpu.SemaphoreType.DMA,
            ],
        ),
        out_shape=[jax.ShapeDtypeStruct((n * rows_each, width), kind) for n, kind in outs],
        compiler_params=pltpu.CompilerParams(vmem_limit_bytes=VMEM_LIMIT),
        cost_estimate=pl.CostEstimate(
            flops=6_000_000_000, bytes_accessed=10_000_000, transcendentals=0
        ),
        name="mix_final",
    )(ids, y, q, fade, gate, gain, near, far, matrix)


def settle_body(residual_ref, kept_ref, near_ref, far_ref, gain_ref, after_ref, norm_ref):
    total = kept_ref[...] + near_ref[...].astype(F32) + far_ref[...].astype(F32)
    after = (residual_ref[...].astype(F32) + total).astype(BF16)
    after_ref[...] = after
    wide = after.astype(F32)
    mean = jnp.mean(wide * wide, axis=-1, keepdims=True)
    norm_ref[...] = (wide * lax.rsqrt(mean + 1e-06) * gain_ref[...].astype(F32)).astype(BF16)


def settle_call(residual, kept, near, far, gain):
    rows, width = residual.shape
    top = pl.BlockSpec((rows // 2, width), lambda i: (i, 0))
    return pl.pallas_call(
        settle_body,
        grid=(2,),
        in_specs=[top] * 4 + [pl.BlockSpec(gain.shape, lambda i: (0, 0))],
        out_specs=[top, top],
        out_shape=[jax.ShapeDtypeStruct(residual.shape, BF16)] * 2,
        compiler_params=pltpu.CompilerParams(vmem_limit_bytes=VMEM_LIMIT),
        name="settle",
    )(residual, kept, near, far, gain)


def finish_body(after_ref, kept_ref, came_ref, l1_ref, l2_ref, r1_ref, r2_ref, out_ref):
    half = l1_ref.shape[1]
    share = kept_ref[...].astype(F32) + came_ref[...].astype(F32)
    left = share[:, :half] + l1_ref[...].astype(F32) + l2_ref[...].astype(F32)
    right = share[:, half:] + r1_ref[...].astype(F32) + r2_ref[...].astype(F32)
    out_ref[:, :half] = (after_ref[:, :half].astype(F32) + 0.5 * left).astype(BF16)
    out_ref[:, half:] = (after_ref[:, half:].astype(F32) + 0.5 * right).astype(BF16)


def finish_call(*arrays):
    rows, width = arrays[0].shape
    each = rows // 2
    return pl.pallas_call(
        finish_body,
        grid=(2,),
        in_specs=[pl.BlockSpec((each, a.shape[1]), lambda i: (i, 0)) for a in arrays],
        out_specs=pl.BlockSpec((each, width), lambda i: (i, 0)),
        out_shape=jax.ShapeDtypeStruct((rows, width), BF16),
        compiler_params=pltpu.CompilerParams(vmem_limit_bytes=VMEM_LIMIT),
        name="finish",
    )(*arrays)


def pick_body(part_ref, gate_ref, up_ref, down_ref, out_ref):
    columns = gate_ref.shape[1]
    for k, ref in enumerate((gate_ref, up_ref, down_ref)):
        out_ref[:, k * columns : (k + 1) * columns] = ref[...]


def pick_call(part, parts, weights):
    rows, columns = weights[0].shape
    columns //= parts
    return pl.pallas_call(
        pick_body,
        grid_spec=pltpu.PrefetchScalarGridSpec(
            num_scalar_prefetch=1,
            grid=(1,),
            in_specs=[pl.BlockSpec((rows, columns), lambda i, part: (0, part[0]))] * 3,
            out_specs=pl.BlockSpec((rows, 3 * columns), lambda i, part: (0, 0)),
        ),
        out_shape=jax.ShapeDtypeStruct((rows, 3 * columns), BF16),
        name="pick",
    )(part, *weights)


def feed_body(place_ref, *refs, pieces):
    own_ref, moved = refs[0], refs[1 : 2 * pieces - 1]
    x_refs = refs[2 * pieces - 1 : -4]
    out_refs, weights, arrived = refs[-4:-2], refs[-2], refs[-1]
    place, odd = place_ref[0], place_ref[1]
    copies = [pltpu.make_async_copy(own_ref, weights.at[0], arrived.at[0])]
    copies[0].start()
    for k in range(1, pieces):
        target = weights.at[k], arrived.at[k]
        copies.append(pltpu.make_async_copy(own_ref, *target))
        for ahead in (True, False):
            steps = k if ahead else pieces - k
            stream, back = moved[2 * steps - 2 : 2 * steps]
            side = place + k < pieces if ahead else place + k >= pieces

            @pl.when(side & (odd == int(ahead)))
            def _(stream=stream, target=target):
                source = stream if len(stream.shape) == 2 else stream.at[0]
                pltpu.make_async_copy(source, *target).start()

            @pl.when(side & (odd != int(ahead)))
            def _(back=back, target=target):
                pltpu.make_async_copy(back, *target).start()

    depth = weights.shape[1]
    columns = weights.shape[2] // 3
    rows = out_refs[0].shape[0]

    def run(k):
        at = lax.rem(place_ref[0] + k, pieces) if pieces > 1 else 0
        return pl.ds(pl.multiple_of(at * depth, depth), depth)

    total = None
    for k, copy in enumerate(copies):
        copy.wait()
        x = jnp.concatenate([x_ref[:, run(k)] for x_ref in x_refs], axis=0)
        term = jnp.dot(x, weights[k, :, : 2 * columns], preferred_element_type=F32)
        total = term if total is None else total + term
    hidden = (silu(total[:, :columns]) * total[:, columns:]).astype(BF16)
    for k in range(pieces):
        product = lax.dot_general(
            hidden,
            weights[k, :, 2 * columns :],
            (((1,), (1,)), ((), ())),
            preferred_element_type=F32,
        ).astype(BF16)
        out_refs[0][:, run(k)] = product[:rows]
        out_refs[1][:, run(k)] = product[rows:]


def feed_call(place, kept, away, weights):
    width = kept[0].shape[1]
    pieces = (len(weights) + 1) // 2
    columns = weights[0].shape[1] // 3
    rows = sum(a.shape[0] for a in kept)
    outs = jax.ShapeDtypeStruct((rows, width), BF16)
    whole = pl.BlockSpec(memory_space=pltpu.VMEM)
    return pl.pallas_call(
        functools.partial(feed_body, pieces=pieces),
        in_specs=[pl.BlockSpec(memory_space=pltpu.SMEM)]
        + [pl.BlockSpec(memory_space=pltpu.HBM)] * len(weights)
        + [whole] * (len(kept) + len(away)),
        out_specs=[whole, whole],
        out_shape=[outs, outs],
        scratch_shapes=[
            pltpu.VMEM((pieces, *weights[0].shape), BF16),
            pltpu.SemaphoreType.DMA((pieces,)),
        ],
        cost_estimate=pl.CostEstimate(
            flops=12 * rows * width * columns, bytes_accessed=8_000_000, transcendentals=0
        ),
        compiler_params=pltpu.CompilerParams(vmem_limit_bytes=3 * VMEM_LIMIT),
        name="feed",
    )(place, *weights, *kept, *away)


def halves(ref, came):
    both = ref.astype(F32) + came.astype(F32)
    half = both.shape[1] // 2
    return both[:, :half].astype(BF16), both[:, half:].astype(BF16)


def feed_forward(x_norm, after_mixer, weights):
    rows, _ = x_norm.shape
    half = rows // 2
    spot = jnp.stack([lax.axis_index("sp"), lax.axis_index("tp") & 1])

    x1 = x_norm
    x_side = swapped(x1, "tp", 2)
    y_side = swapped(x1, "grp", 1)
    x1_away = swapped(x1, "tp", 1)
    corner_top = swapped(y_side[:half], "tp", 2)
    corner_low = swapped(x_side[half:], "grp", 1)
    x_away = swapped(x_side, "tp", 1)
    y_away = swapped(y_side, "tp", 1)
    top_away = swapped(corner_top, "tp", 1)
    low_away = swapped(corner_low, "tp", 1)

    def feed(kept, away):
        mine, theirs = feed_call(spot, kept, away, weights)
        return mine, swapped(theirs, "tp", 1)

    own, own_came = feed([x1], [x1_away])
    xs, xs_came = feed([x_side], [x_away])
    corner, corner_came = feed([corner_top, corner_low], [top_away, low_away])
    ys, ys_came = feed([y_side], [y_away])
    x_left, x_right = halves(xs, xs_came)
    y_left, y_right = halves(ys, ys_came)
    l1 = swapped(x_left, "tp", 2)
    r1 = swapped(y_right, "grp", 1)
    c_left, c_right = halves(corner, corner_came)
    l2 = swapped(c_left, "tp", 2)
    r2 = swapped(c_right, "grp", 1)
    y_left = (y_left.astype(F32) + l2.astype(F32)).astype(BF16)
    x_right = (x_right.astype(F32) + r2.astype(F32)).astype(BF16)
    l2 = swapped(y_left, "grp", 1)
    r2 = swapped(x_right, "tp", 2)
    return finish_call(after_mixer, own, own_came, l1, l2, r1, r2)


def feed_forward_any(x_norm, after_mixer, weights):
    (weight,) = weights
    columns = weight.shape[1] // 3
    x = lax.all_gather(x_norm, ("grp", "tp"), axis=0, tiled=True)
    gates = jnp.dot(x, weight[:, :columns], preferred_element_type=F32)
    ups = jnp.dot(x, weight[:, columns : 2 * columns], preferred_element_type=F32)
    hidden = (silu(gates) * ups).astype(BF16)
    share = lax.dot_general(
        hidden,
        weight[:, 2 * columns :],
        (((1,), (1,)), ((), ())),
        preferred_element_type=F32,
    ).astype(BF16)
    share = lax.psum_scatter(share, ("grp", "tp"), scatter_dimension=0, tiled=True)
    return (after_mixer.astype(F32) + 0.5 * share.astype(F32)).astype(BF16)


def shifted(value, axis, steps):
    count = lax.axis_size(axis)
    return lax.ppermute(value, axis, [(s, s + steps) for s in range(count - steps)])


def either_way(value):
    count, members = lax.axis_size("sp"), lax.axis_size("tp")
    pairs = []
    for s in range(count):
        for t in range(members):
            target = s - 1 if t % 2 else s + 1
            if 0 <= target < count:
                pairs.append((s * members + t, target * members + t))
    return lax.ppermute(value, ("sp", "tp"), pairs)


def swapped(value, axis, bit):
    count = lax.axis_size(axis)
    return lax.ppermute(value, axis, [(s, s ^ bit) for s in range(count)])


def entering_states(packed, axis):
    count = lax.axis_size(axis)
    window, before, got = packed, None, jnp.zeros_like(packed)
    reach = 1
    while reach < count:
        if reach > 1:
            window = join_call(window, got)
            before = got if before is None else join_call(before, got)
        got = shifted(window, axis, reach)
        reach *= 2
    return (got, jnp.zeros_like(got)) if before is None else (before, got)


def on_device(
    residual,
    value_projected,
    gate_projected,
    wide_key_rows,
    wide_query_rows,
    narrow_key_rows,
    narrow_query_rows,
    step_before_softplus,
    extra_log_decay,
    log_decay_rate,
    value_kernel,
    wide_key_kernel,
    wide_query_kernel,
    narrow_key_kernel,
    narrow_query_kernel,
    head_norm_gain,
    output_matrix,
    feedforward_norm_gain,
    gate_matrix,
    up_matrix,
    down_matrix,
):
    members = lax.axis_size("tp")
    place = lax.axis_index("tp")
    part = jnp.reshape(lax.axis_index("grp"), (1,))
    mine = pick_call(part, lax.axis_size("grp"), (gate_matrix, up_matrix, down_matrix))
    raw = (value_projected, wide_key_rows, wide_query_rows, narrow_key_rows, narrow_query_rows)
    rim = shifted(tails_call(raw), "sp", 1)
    count = lax.axis_size("sp")
    direct = members == 4 and lax.axis_size("grp") == 2 and count == 4
    if direct:
        mine, rim = lax.optimization_barrier((mine, rim))
        first = either_way(mine)
    else:
        weights = [lax.all_gather(mine, "sp", axis=0, tiled=True)]

    taps = (
        value_kernel,
        wide_key_kernel,
        wide_query_kernel,
        narrow_key_kernel,
        narrow_query_kernel,
    )
    y, q, fade, packed = local_call(
        raw, step_before_softplus.T, extra_log_decay.T, log_decay_rate[None, :], rim, taps
    )
    if direct:
        mine, packed = lax.optimization_barrier((mine, packed))
    near, far = entering_states(packed, "sp")
    if direct:
        pair = jnp.stack([first, swapped(mine, "tp", 1)])
    if direct:
        pair, near, far = lax.optimization_barrier((pair, near, far))
        streams = [first]
        backs = []
        for k in range(2, count + 1):
            pair = either_way(pair if k < count else pair[1])
            if k < count:
                streams.append(pair)
            backs.append(swapped(pair[1] if k < count else pair, "tp", 1))
        weights = [mine]
        for stream, back in zip(streams, backs):
            weights += [stream, back]

    rows = y.shape[0] // members
    masks = 2 * jnp.arange(members // 2, dtype=jnp.int32)
    shared = (y, q, fade, gate_projected, head_norm_gain[None, :], near, far, output_matrix, rows)
    half = members // 2
    ids = jnp.concatenate([(place ^ 1) ^ masks, place ^ masks[1:]])
    away, far_kept = final_call(ids, *shared, [(half, BF16), (half - 1, BF16)])
    came = swapped(away, "tp", 1)
    (kept,) = final_call(place ^ masks[:1], *shared, [(1, F32)])
    bit = members // 2
    total = {}

    def block(array, index):
        return array[index * rows : (index + 1) * rows]

    for mask in range(2, members, 2):
        total[mask] = block(far_kept, mask // 2 - 1).astype(F32) + block(came, mask // 2).astype(F32)
    last = None
    while bit > 1:
        for mask in range(0, bit, 2):
            got = swapped(total[mask + bit].astype(BF16), "tp", bit)
            if mask == 0:
                last = got if last is None else last.astype(F32) + got.astype(F32)
            else:
                total[mask] = total[mask] + got.astype(F32)
        bit //= 2
    after_mixer, x_norm = settle_call(residual, kept, came, last, feedforward_norm_gain[None, :])
    if members == 4 and lax.axis_size("grp") == 2:
        return feed_forward(x_norm, after_mixer, weights)
    return feed_forward_any(x_norm, after_mixer, weights)


def solution(mesh):
    in_specs = (
        P(("grp", "sp", "tp"), None),
        P(("grp", "sp"), "tp"),
        P(("grp", "sp"), "tp"),
        P(("grp", "sp"), "tp"),
        P(("grp", "sp"), "tp"),
        P(("grp", "sp"), "tp"),
        P(("grp", "sp"), "tp"),
        P(("grp", "sp"), "tp"),
        P(("grp", "sp"), "tp"),
        P("tp"),
        P(None, "tp"),
        P(None, "tp"),
        P(None, "tp"),
        P(None, "tp"),
        P(None, "tp"),
        P("tp"),
        P("tp", None),
        P(),
        P("sp", "tp"),
        P("sp", "tp"),
        P("sp", "tp"),
    )
    out_specs = P(("grp", "sp", "tp"), None)

    return jax.shard_map(
        on_device, mesh=mesh, in_specs=in_specs, out_specs=out_specs, check_vma=False
    )
```
